512 devices in a mesh: sp: 32 (over z, x), tp: 16 (over y, core).
Axes of the slice: x: 4, y: 8, z: 8, core: 2. Of those that a mesh axis runs over, the one named last changes fastest.
Arguments:
- stream_in: bfloat16 [8192, 2048], P(('sp', 'tp')), may hold values from -6 to 6
- pre_gate: bfloat16 [8192, 1024], P('sp', 'tp'), may hold values from -6 to 6
- value_in: bfloat16 [8192, 1024], P('sp', 'tp'), may hold values from -6 to 6
- post_gate: bfloat16 [8192, 1024], P('sp', 'tp'), may hold values from -6 to 6
- conv_taps: bfloat16 [3, 1024], P(None, 'tp'), may hold values from -3 to 3
- out_weight: bfloat16 [1024, 2048], P('tp'), may hold values from -0.1875 to 0.1875
- route_ids: int32 [8192, 4], P('sp'), may hold values from 0 to 31, all different within a row; in each aligned block of 16 rows (0 to 15, 16 to 31, ...) at most 4 rows name the same one
- route_weight: float32 [8192, 4], P('sp'), may hold values from 0.1 to 1
- ffn_gain: bfloat16 [2048], replicated, may hold values from 0.099609375 to 1.8984375
- post_gain: bfloat16 [2048], replicated, may hold values from 0.099609375 to 1.8984375
- gate_proj: bfloat16 [32, 2048, 2048], P('sp', None, 'tp'), may hold values from -0.39648438 to 0.39648438
- up_proj: bfloat16 [32, 2048, 2048], P('sp', None, 'tp'), may hold values from -0.39648438 to 0.39648438
- down_proj: bfloat16 [32, 2048, 2048], P('sp', None, 'tp'), may hold values from -0.125 to 0.125
Outputs:
- layer_out: bfloat16 [8192, 2048], P(('sp', 'tp'))
The draws below stay inside these ranges and needn't reach their ends.
Inputs may be any that keep to these rules, and one draw needn't show every extreme that they name: `route_ids`: in each aligned block of 16 positions, a row names 4 different experts and no expert is named by more than 4 rows; in every draw some expert reaches 4 in some block.
All inputs are finite; a program needn't handle non-finite values.
Results may differ from the reference program's by a relative error of at most 0.014.
Values may be sent and summed in bfloat16 or wider, within the bound.
A program may use at most 64 MiB of HBM per device.

```python
import math
import jax
import jax.numpy as jnp
import numpy as np
from jax import lax

D = 2048
W = 1024
FF = 2048
TOPK = 4
KERNEL = 3
TOKENS = 8192
EXPERTS = 32
ROWS = 16
CAP = 4
SLOTS = 2048


def shard_levels(key, extent, shards, low, top_value):
    level, own = 1.0, jax.random.fold_in(key, 6)
    for position, blocks in shards:
        heights = jnp.exp(jax.random.uniform(jax.random.fold_in(own, position), (blocks,), jnp.float32, low / len(shards), top_value / len(shards)))
        level = level * jnp.repeat(heights, extent[position] // blocks).reshape([-1 if axis == position else 1 for axis in range(len(extent))])
    return level


def deal_out(stream_key, own, number, rows, count, top, bound, slope):
    sequence = jax.random.permutation(stream_key, count)
    crowded, ordinary = load_shares(count, rows * top, bound, slope, True), load_shares(count, rows * top, bound, slope, False)
    places = jnp.arange(count)

    def named(lengths, rotation):
        used = int((lengths > 0).sum())
        fixed = max(1, used // 4)
        moved = fixed + (places - fixed + rotation * (used - fixed)) % max(1, count - fixed)
        return jnp.zeros((count,), jnp.int32).at[sequence[jnp.where(places < fixed, places, moved)]].set(jnp.asarray(lengths, jnp.int32))

    lengths = jnp.where(number % 4 == 0, named(crowded, number // 4), named(ordinary, number - number // 4 - 1))
    mixed = jax.random.permutation(jax.random.fold_in(own, 3), count)
    donor, receiver = mixed[0:count // 2 * 2:2], mixed[1:count // 2 * 2:2]
    margin = jnp.minimum(lengths[donor] - 1, bound - lengths[receiver]) // 2
    margin = jnp.where((donor == sequence[0]) | (receiver == sequence[0]) | (lengths[receiver] == 0), 0, jnp.maximum(margin, 0))
    moved = jax.random.randint(jax.random.fold_in(own, 4), (count // 2,), 0, 1 << 20) % (margin + 1)
    lengths = lengths.at[donor].add(-moved).at[receiver].add(moved)
    members = jnp.searchsorted(jnp.cumsum(lengths), jnp.arange(rows * top), side="right").astype(jnp.int32)
    grid = members.reshape(top, rows).T
    grid = grid[jax.random.permutation(jax.random.fold_in(own, 1), rows)]
    rotation = jax.random.randint(jax.random.fold_in(own, 2), (rows, 1), 0, top)
    return jnp.take_along_axis(grid, (jnp.arange(top)[None, :] + rotation) % top, axis=1)


def load_shares(number_of, total, bound, lean, full):
    portions = [(1 << 20) // math.isqrt(standing ** lean) + 1 for standing in range(1, number_of + 1)]
    largest = bound if full else min(bound, max(-(-total // number_of), total * portions[0] // sum(portions)))
    least = 1 if total - largest >= number_of - 1 else 0
    counts, rest = [largest] + [least] * (number_of - 1), total - largest - least * (number_of - 1)
    while rest > 0:
        candidates = [i for i in range(1, number_of) if counts[i] < largest] or [i for i in range(1, number_of) if counts[i] < bound]
        whole, remaining = sum([portions[i] for i in candidates]), rest
        for i in candidates:
            addition = min(bound - counts[i], max(1, remaining * portions[i] // whole), rest)
            counts[i] = counts[i] + addition
            rest = rest - addition
    return np.array(counts)


def normal_values(rng, extent, width, limit, split=(), kind=jnp.bfloat16):
    drawn = width * jax.random.normal(rng, extent, jnp.float32)
    if split:
        drawn = drawn * shard_levels(rng, extent, split, -0.22, 0.18)
    return jnp.clip(drawn, -limit, limit).astype(kind)


def setup_inputs(seed: int = 0) -> dict:
    key_of = jax.random.split(jax.random.key(seed), 14)
    stream_in = normal_values(key_of[0], (TOKENS, D), 1.0, 6.0, ((0, 512),))
    pre_gate = normal_values(key_of[1], (TOKENS, W), 1.0, 6.0, ((0, 32), (1, 16)))
    value_in = normal_values(key_of[2], (TOKENS, W), 1.0, 6.0, ((0, 32), (1, 16)))
    post_gate = normal_values(key_of[3], (TOKENS, W), 1.0, 6.0, ((0, 32), (1, 16)))
    conv_taps = normal_values(key_of[4], (KERNEL, W), 0.6, 3.0, ((1, 16),))
    out_weight = normal_values(key_of[5], (W, D), W ** -0.5, 0.1875, ((0, 16),))
    route_ids_keys = jax.random.split(jax.random.fold_in(key_of[6], 1), TOKENS // ROWS)
    route_ids_turns = jax.random.permutation(jax.random.fold_in(key_of[6], 3), TOKENS // ROWS)
    route_ids = jax.vmap(lambda own, number: deal_out(jax.random.fold_in(key_of[6], 2), own, number, ROWS, EXPERTS, TOPK, CAP, 2))(route_ids_keys, route_ids_turns).reshape((TOKENS, TOPK))
    route_weight = jnp.clip(jnp.exp(math.log(1.0) - 2.3025851 * jax.random.uniform(key_of[7], (TOKENS, TOPK), jnp.float32) ** shard_levels(key_of[7], (TOKENS, TOPK), ((0, 32),), -0.2, 0.2)), 0.1, 1.0)
    ffn_gain = jnp.clip(1.0 + 0.18 * jax.random.normal(key_of[8], (D,), jnp.float32), 0.099609375, 1.8984375).astype(jnp.bfloat16)
    post_gain = jnp.clip(1.0 + 0.18 * jax.random.normal(key_of[9], (D,), jnp.float32), 0.099609375, 1.8984375).astype(jnp.bfloat16)
    gate_proj = normal_values(key_of[10], (EXPERTS, D, FF), (3.0 * D ** -0.5), 0.39648438, ((0, 32), (2, 16)))
    up_proj = normal_values(key_of[11], (EXPERTS, D, FF), (3.0 * D ** -0.5), 0.39648438, ((0, 32), (2, 16)))
    down_proj = normal_values(key_of[12], (EXPERTS, FF, D), FF ** -0.5, 0.125, ((0, 32), (2, 16)))
    return dict(stream_in=stream_in, pre_gate=pre_gate, value_in=value_in, post_gate=post_gate, conv_taps=conv_taps, out_weight=out_weight, route_ids=route_ids, route_weight=route_weight, ffn_gain=ffn_gain, post_gain=post_gain, gate_proj=gate_proj, up_proj=up_proj, down_proj=down_proj)


clamp_limit = 7.0
sigmoid_scale = 1.702
epsilon = 1e-06

def clamped_units(gate_pre, up_pre):
    gate_cut = jnp.minimum(gate_pre, clamp_limit)
    up_cut = jnp.clip(up_pre, -clamp_limit, clamp_limit)
    return (up_cut + 1.0) * (gate_cut * jax.nn.sigmoid(sigmoid_scale * gate_cut))

def scaled_norm(values, gain):
    return values * lax.rsqrt(lax.optimization_barrier(jnp.mean(values * values, axis=-1, keepdims=True)) + epsilon) * gain.astype(jnp.float32)

def reference(stream_in, pre_gate, value_in, post_gate, conv_taps, out_weight, route_ids, route_weight, ffn_gain, post_gain, gate_proj, up_proj, down_proj):
    tap_count = conv_taps.shape[0]
    gated_input = (pre_gate.astype(jnp.float32) * value_in.astype(jnp.float32)).astype(jnp.bfloat16)
    padded = jnp.concatenate([jnp.zeros((tap_count - 1, W), jnp.bfloat16), gated_input], 0).astype(jnp.float32)
    convolved = jnp.zeros((TOKENS, W), jnp.float32)
    for tap_index in range(tap_count):
        convolved = convolved + conv_taps[tap_index].astype(jnp.float32)[None, :] * padded[tap_index:tap_index + TOKENS]
    mixer_out = (post_gate.astype(jnp.float32) * convolved).astype(jnp.bfloat16)
    projected = jnp.dot(mixer_out, out_weight, preferred_element_type=jnp.float32)
    residual = (stream_in.astype(jnp.float32) + projected).astype(jnp.bfloat16)
    normed = scaled_norm(residual.astype(jnp.float32), ffn_gain).astype(jnp.bfloat16)
    flattened = route_ids.reshape(-1).astype(jnp.int32)
    entries = flattened.shape[0]
    onehot = (flattened[:, None] == jnp.arange(EXPERTS, dtype=jnp.int32)[None, :]).astype(jnp.int32)
    blocked = onehot.reshape(entries // (ROWS * TOPK), ROWS * TOPK, EXPERTS)
    before = jnp.cumsum(blocked, axis=1) - blocked
    slot_rank = lax.optimization_barrier(jnp.sum(before * blocked, axis=2)).reshape(entries)
    block_ids = jnp.arange(entries, dtype=jnp.int32) // (ROWS * TOPK)
    slot_index = (block_ids * CAP + slot_rank).astype(jnp.int32)
    token_ids = jnp.arange(entries, dtype=jnp.int32) // TOPK
    slot_table = jnp.full((EXPERTS, SLOTS), TOKENS, jnp.int32).at[flattened, slot_index].set(token_ids)
    padded_rows = jnp.concatenate([normed, jnp.zeros((1, D), jnp.bfloat16)], 0)

    def one_expert(packed):
        token_rows, gate_matrix, up_matrix, down_matrix = packed
        inputs = padded_rows[token_rows]
        gate_pre = jnp.dot(inputs, gate_matrix, preferred_element_type=jnp.float32)
        up_pre = jnp.dot(inputs, up_matrix, preferred_element_type=jnp.float32)
        hidden = clamped_units(gate_pre, up_pre).astype(jnp.bfloat16)
        return jnp.dot(hidden, down_matrix, preferred_element_type=jnp.float32).astype(jnp.bfloat16)
    expert_outs = lax.map(one_expert, (slot_table, gate_proj, up_proj, down_proj))
    picked = expert_outs[flattened, slot_index].astype(jnp.float32).reshape(TOKENS, TOPK, D)
    combined = lax.optimization_barrier(jnp.sum(picked * route_weight[:, :, None], axis=1)).astype(jnp.bfloat16)
    layer_out = residual.astype(jnp.float32) + scaled_norm(combined.astype(jnp.float32), post_gain)
    return layer_out.astype(jnp.bfloat16)
```

```python
import functools

import jax
import jax.numpy as jnp
from jax import lax
from jax.experimental import pallas as pl
from jax.experimental.pallas import tpu as pltpu
from jax.sharding import PartitionSpec as P

MESH = pl.DeviceIdType.MESH
F32 = jnp.float32
BF16 = jnp.bfloat16
LIMIT = 7.0
SLOPE = 1.702
EPS = 1e-06
CHUNKS = 4
OPS = (("r", 0), ("r", 1), ("r", 2), ("h", 0), ("r", 3), ("h", 1), ("h", 2), ("h", 3))


def kernel(
    cfg,
    stream, pre, value, post, taps, weight, ids, route_w, ffn_gain, post_gain,
    gate_hbm, up_hbm, down_hbm,
    out,
    halo_src, halo_dst, mixed, w_in, w_diag, s_in, squares, picker, comb_w, slot_cols,
    sent, rows, hidden, result, back, res_keep, res_in, comb_out, comb_in, w_gu, w_down,
    load_sem, halo_sem, small_send, small_recv, mix_recv, disp_recv, ring_recv, ring_pair,
    ring_send, back_recv,
):
    n_sp, n_tp, dim_x, cap = cfg
    dim_z, dim_y = n_sp // dim_x, n_tp // 2
    s, t = lax.axis_index("sp"), lax.axis_index("tp")
    sz, sx = s // dim_x, lax.rem(s, dim_x)
    y, core = t // 2, lax.rem(t, 2)
    n_rows = pre.shape[0]
    own = n_rows // n_tp
    half = n_rows // 2
    block = own * cap * n_tp // own
    slots = block * n_sp
    per_chunk = n_sp // CHUNKS
    chunk = per_chunk * block

    def at_tp(step_y, other_core):
        to_core = 1 - core if other_core else core
        return lax.rem(y + step_y + dim_y, dim_y) * 2 + to_core

    def remote(src, dst, send, recv, tp=None, sp=None):
        target = {"tp": tp} if sp is None else {"sp": sp}
        return pltpu.make_async_remote_copy(
            src_ref=src, dst_ref=dst, send_sem=send, recv_sem=recv,
            device_id=target, device_id_type=MESH,
        )

    def drain(ref, sem):
        pltpu.make_async_copy(ref, ref, sem).wait()

    def z_step(p):
        place = p // dim_x
        return (place + 1) // 2 if place % 2 else (dim_z - place // 2) % dim_z

    loads = [
        pltpu.make_async_copy(gate_hbm.at[0], w_gu.at[:, pl.ds(0, 128)], load_sem.at[0]),
        pltpu.make_async_copy(up_hbm.at[0], w_gu.at[:, pl.ds(128, 128)], load_sem.at[1]),
        pltpu.make_async_copy(down_hbm.at[0], w_down, load_sem.at[2]),
    ]
    for load in loads:
        load.start()

    barrier = pltpu.get_barrier_semaphore()

    def greet_tp(step, carry):
        pl.semaphore_signal(
            barrier, inc=1, device_id={"tp": lax.rem(t + step, n_tp)}, device_id_type=MESH
        )
        return carry

    def greet_sp(step, carry):
        pl.semaphore_signal(
            barrier, inc=1, device_id={"sp": lax.rem(s + step, n_sp)}, device_id_type=MESH
        )
        return carry

    lax.fori_loop(1, n_tp, greet_tp, 0)
    lax.fori_loop(1, n_sp, greet_sp, 0)

    gated = (pre[...].astype(F32) * value[...].astype(F32)).astype(BF16)
    halo_src[:, pl.ds(0, gated.shape[1])] = gated[n_rows - 16 :, :]
    w_diag[...] = jnp.zeros_like(w_diag)

    pl.semaphore_wait(barrier, n_tp + n_sp - 2)

    halo = remote(
        halo_src, halo_dst, halo_sem.at[0], halo_sem.at[1], sp=lax.rem(s + 1, n_sp)
    )
    halo.start()

    tp_steps = [(d, o) for d in (4, 3, 5, 2, 6, 1, 7) for o in (False, True)] + [(0, True)]
    for step_y, other in tp_steps:
        to = at_tp(step_y, other)
        piece = pl.ds(pl.multiple_of(to * 128, 128), 128)
        remote(weight.at[:, piece], w_in.at[t], small_send.at[0], small_recv.at[0], tp=to).start()
    for step_y, other in tp_steps:
        to = at_tp(step_y, other)
        piece = pl.ds(pl.multiple_of(to * 128, 128), 128)
        remote(stream.at[:, piece], s_in.at[t], small_send.at[1], small_recv.at[1], tp=to).start()
    own_cols = pl.ds(pl.multiple_of(t * 128, 128), 128)
    w_in[t] = weight[:, own_cols]
    s_in[t] = stream[:, own_cols]

    wide = gated.astype(F32)
    tap = taps[...].astype(F32)
    row_no = lax.broadcasted_iota(jnp.int32, wide.shape, 0)
    shift_1, shift_2 = pltpu.roll(wide, 1, 0), pltpu.roll(wide, 2, 0)
    halo.wait_recv()
    rim = halo_dst[...].astype(F32)[:, : wide.shape[1]]
    rim = jnp.where(s > 0, rim, 0.0)
    last, before_last = rim[15:16, :], rim[14:15, :]
    shift_1 = jnp.where(row_no == 0, last, shift_1)
    shift_2 = jnp.where(row_no == 0, before_last, jnp.where(row_no == 1, last, shift_2))
    convolved = tap[0:1] * shift_2
    convolved = convolved + tap[1:2] * shift_1
    convolved = convolved + tap[2:3] * wide
    mixer = post[...].astype(F32) * convolved
    mixed[t] = jnp.concatenate([mixer[:half], mixer[half:]], axis=1).astype(BF16)

    steps = (4, 3, 5, 2, 6, 1, 7)
    for step_y in steps:
        remote(
            mixed.at[t], mixed.at[t], small_send.at[2], mix_recv.at[step_y], tp=at_tp(step_y, False)
        ).start()
    partner = at_tp(0, True)
    remote(mixed.at[t], mixed.at[t], small_send.at[2], mix_recv.at[0], tp=partner).start()

    id_cols = ids[...]
    lane = lax.broadcasted_iota(jnp.int32, (n_rows, 128), 1)
    named = jnp.zeros((n_rows, 128), F32)
    for k in range(ids.shape[1]):
        named = named + jnp.where(id_cols[:, k : k + 1] == lane, 1.0, 0.0)
    row_a = lax.broadcasted_iota(jnp.int32, (n_rows, n_rows), 0)
    row_b = lax.broadcasted_iota(jnp.int32, (n_rows, n_rows), 1)
    earlier = jnp.where((row_a > row_b) & (row_a // own == row_b // own), 1.0, 0.0).astype(BF16)
    rank = jnp.dot(earlier, named.astype(BF16), preferred_element_type=F32).astype(jnp.int32)
    dz = lax.rem(sz - lane // dim_x + 32 * dim_z, dim_z)
    dx = lax.rem(sx - lax.rem(lane, dim_x) + 32 * dim_x, dim_x)
    z_place = jnp.where(
        dz * 2 <= dim_z, jnp.maximum(2 * dz - 1, 0), 2 * (dim_z - dz)
    )
    at_lane = lax.broadcasted_iota(jnp.int32, (n_rows, 128), 0)
    slot_of = ((z_place * dim_x + dx) * block + (at_lane // own) * cap + rank).astype(F32)
    columns = jnp.zeros((n_rows, 128), F32)
    for k in range(ids.shape[1]):
        found = jnp.sum(
            jnp.where(id_cols[:, k : k + 1] == lane, slot_of, 0.0), axis=1, keepdims=True
        )
        columns = jnp.where(lane == k, found, columns)
    slot_cols[...] = columns
    slot_rows = jnp.transpose(columns)

    def fill_picker(part, carry):
        first = pl.multiple_of(part * 256, 256)
        number = lax.broadcasted_iota(jnp.int32, (256, n_rows), 0) + part * 256
        number = number.astype(F32)
        hit = number == slot_rows[0:1, :]
        for k in range(1, ids.shape[1]):
            hit = hit | (number == slot_rows[k : k + 1, :])
        picker[pl.ds(first, 256), :] = jnp.where(hit, 1.0, 0.0).astype(BF16)
        return carry

    lax.fori_loop(0, slots // 256, fill_picker, 0)

    drain(w_in.at[pl.ds(0, n_tp - 1)], small_recv.at[0])
    for k in range(n_tp):
        piece = w_in[k]
        w_diag[pl.ds(k * 128, 64), pl.ds(0, 128)] = piece
        w_diag[pl.ds(k * 128 + 64, 64), pl.ds(128, 128)] = piece
    for step_y in steps:
        arrived = mixed.at[at_tp(-step_y, False)]
        drain(arrived, mix_recv.at[step_y])
        remote(arrived, arrived, small_send.at[2], mix_recv.at[0], tp=partner).start()
    drain(s_in.at[pl.ds(0, n_tp - 1)], small_recv.at[1])
    drain(mixed.at[pl.ds(0, dim_y)], mix_recv.at[0])
    stacked = jnp.concatenate([mixed[k] for k in range(n_tp)], axis=1)
    projected = jnp.dot(stacked, w_diag[...], preferred_element_type=F32)
    projected = jnp.concatenate([projected[:, :128], projected[:, 128:]], axis=0)
    residual = (s_in[...].reshape(n_rows, 128).astype(F32) + projected).astype(BF16)
    res_keep[...] = residual
    res = residual.astype(F32)

    sums = jnp.sum(res * res, axis=1, keepdims=True)
    across = jnp.transpose(jnp.broadcast_to(sums, (n_rows, 128)))
    first_row = lax.broadcasted_iota(jnp.int32, (8, half), 0) == 0
    squares[t] = jnp.where(first_row, across[0:8, :half], across[0:8, half:])
    for step_y, other in tp_steps:
        remote(
            squares.at[t], squares.at[t], small_send.at[3], small_recv.at[2],
            tp=at_tp(step_y, other),
        ).start()
    for step_y, other in tp_steps:
        to = at_tp(step_y, other)
        remote(
            res_keep.at[pl.ds(pl.multiple_of(to * own, own), own), :], res_in.at[t],
            small_send.at[4], small_recv.at[3], tp=to,
        ).start()
    res_in[t] = res_keep[pl.ds(pl.multiple_of(t * own, own), own), :]
    drain(squares.at[pl.ds(0, n_tp - 1)], small_recv.at[2])
    total = squares[0]
    for k in range(1, n_tp):
        total = total + squares[k]
    scale = lax.rsqrt(total / (n_tp * 128) + EPS)
    scale = jnp.concatenate(
        [jnp.transpose(jnp.broadcast_to(scale[k : k + 1, :], (half, half))) for k in range(2)], axis=0
    )
    normed = (res * scale * ffn_gain[:, own_cols].astype(F32)).astype(BF16)

    for part in range(CHUNKS):
        span = pl.ds(part * chunk, chunk)
        picked = jnp.dot(picker[span, :], normed, preferred_element_type=F32).astype(BF16)
        sent[span, :] = picked
        if part == 0:
            rows[t, pl.ds(0, block), :] = picked[:block]
        for p in range(max(1, part * per_chunk), (part + 1) * per_chunk):
            to_z = lax.rem(sz - z_step(p) + dim_z, dim_z)
            to_x = lax.rem(sx - p % dim_x + dim_x, dim_x)
            place = pl.ds(p * block, block)
            remote(
                sent.at[place, :], rows.at[t, place, :], small_send.at[5], disp_recv.at[part],
                sp=to_z * dim_x + to_x,
            ).start()

    def fill_weights(part, carry):
        first = pl.multiple_of(part * 256, 256)
        number = lax.broadcasted_iota(jnp.int32, (n_rows, 256), 1) + part * 256
        number = number.astype(F32)
        places = slot_cols[...]
        amounts = route_w[...]
        summed = jnp.zeros((n_rows, 256), F32)
        for k in range(ids.shape[1]):
            summed = summed + jnp.where(
                number == places[:, k : k + 1], amounts[:, k : k + 1], 0.0
            )
        high = summed.astype(BF16)
        comb_w[pl.ds(0, n_rows), pl.ds(first, 256)] = high
        comb_w[pl.ds(n_rows, n_rows), pl.ds(first, 256)] = (summed - high.astype(F32)).astype(BF16)
        return carry

    lax.fori_loop(0, slots // 256, fill_weights, 0)
    for load in loads:
        load.wait()

    lower, upper = chunk // 2, chunk - chunk // 2

    def units(i, part):
        span = pl.ds(i * chunk + part * lower, lower)
        held = jnp.concatenate([rows[k, span, :] for k in range(n_tp)], axis=1)
        both = jnp.dot(held, w_gu[...], preferred_element_type=F32)
        gate = jnp.minimum(both[:, :128], LIMIT)
        up = jnp.clip(both[:, 128:], -LIMIT, LIMIT)
        hidden[t, span, :] = ((up + 1.0) * (gate * jax.nn.sigmoid(SLOPE * gate))).astype(BF16)

    def outputs(i, part):
        span = pl.ds(i * chunk + part * lower, lower)
        held = jnp.concatenate([hidden[k, span, :] for k in range(n_tp)], axis=1)
        result[span, :] = jnp.dot(held, w_down[...], preferred_element_type=F32).astype(BF16)

    def send_back(i):
        for p in range(i * per_chunk, (i + 1) * per_chunk):
            place = pl.ds(p * block, block)
            if p == 0:
                back[place, :] = result[place, :]
                continue
            to_z = lax.rem(sz + z_step(p), dim_z)
            to_x = lax.rem(sx + p % dim_x, dim_x)
            remote(
                result.at[place, :], back.at[place, :], small_send.at[6], back_recv.at[i],
                sp=to_z * dim_x + to_x,
            ).start()

    right, left = at_tp(1, False), at_tp(-1, False)

    def ring_step(j, d):
        kind, i = OPS[j]
        held = rows if kind == "r" else hidden
        full = pl.ds(i * chunk, chunk)
        first = pl.ds(i * chunk, lower)
        second = pl.ds(i * chunk + lower, upper)

        def pass_on(origin, span, to, sem):
            piece = held.at[origin, span, :]
            remote(piece, piece, ring_send.at[j], sem, tp=to).start()

        if d == 0:
            if kind == "r":
                taken = (per_chunk - (1 if i == 0 else 0)) * block
                drain(sent.at[pl.ds(0, taken), :], disp_recv.at[i])
            pass_on(t, full, right, ring_recv.at[j, 0, 0])
            pass_on(t, full, left, ring_recv.at[j, 1, 0])
            pass_on(t, full, partner, ring_pair.at[j])
            return
        for way, sign, ahead, end in ((0, -1, right, first), (1, 1, left, second)):
            origin = at_tp(sign * d, False)
            span = full if d < 4 else end
            drain(held.at[origin, span, :], ring_recv.at[j, way, d - 1])
            if d < 4:
                pass_on(origin, full if d < 3 else end, ahead, ring_recv.at[j, way, d])
            pass_on(origin, span, partner, ring_pair.at[j])
        if d == 4:
            drain(held.at[pl.ds(0, dim_y), full, :], ring_pair.at[j])

    work = {
        4: [(units, 0, 0)], 5: [(units, 0, 1)],
        7: [(units, 1, 0)], 8: [(units, 1, 1)],
        9: [(units, 2, 0)],
        10: [(outputs, 0, 0), (outputs, 0, 1)],
        11: [(units, 2, 1)],
        12: [(units, 3, 0)], 13: [(units, 3, 1)],
        14: [(outputs, 1, 0), (outputs, 1, 1)],
        16: [(outputs, 2, 0), (outputs, 2, 1)],
        18: [(outputs, 3, 0), (outputs, 3, 1)],
    }
    for slot in range(2 * len(OPS) + 3):
        for j in range(len(OPS)):
            d = slot - 2 * j
            if 0 <= d <= 4:
                ring_step(j, d)
        for task, i, part in work.get(slot, ()):
            task(i, part)
            if task is outputs and part == 1:
                send_back(i)

    summed = jnp.zeros((2 * n_rows, 128), F32)
    for i in range(CHUNKS):
        taken = (per_chunk - (1 if i == 0 else 0)) * block
        drain(back.at[pl.ds(0, taken), :], back_recv.at[i])
        span = pl.ds(i * chunk, chunk)
        summed = summed + jnp.dot(comb_w[:, span], back[span, :], preferred_element_type=F32)
    comb_out[...] = (summed[:n_rows] + summed[n_rows:]).astype(BF16)
    for step_y, other in tp_steps:
        to = at_tp(step_y, other)
        remote(
            comb_out.at[pl.ds(pl.multiple_of(to * own, own), own), :], comb_in.at[t],
            small_send.at[7], small_recv.at[4], tp=to,
        ).start()
    comb_in[t] = comb_out[pl.ds(pl.multiple_of(t * own, own), own), :]

    halo.wait_send()
    drain(w_in.at[pl.ds(0, n_tp - 1)], small_send.at[0])
    drain(s_in.at[pl.ds(0, n_tp - 1)], small_send.at[1])
    drain(mixed.at[pl.ds(0, 2 * dim_y - 1)], small_send.at[2])
    drain(squares.at[pl.ds(0, n_tp - 1)], small_send.at[3])
    drain(res_in.at[pl.ds(0, n_tp - 1)], small_send.at[4])
    drain(sent.at[pl.ds(0, slots - block), :], small_send.at[5])
    drain(result.at[pl.ds(0, slots - block), :], small_send.at[6])
    for j in range(len(OPS)):
        drain(rows.at[pl.ds(0, 15), pl.ds(0, chunk), :], ring_send.at[j])

    drain(res_in.at[pl.ds(0, n_tp - 1)], small_recv.at[3])
    drain(comb_in.at[pl.ds(0, n_tp - 1)], small_recv.at[4])
    drain(comb_in.at[pl.ds(0, n_tp - 1)], small_send.at[7])
    combined = jnp.concatenate([comb_in[k] for k in range(n_tp)], axis=1).astype(F32)
    kept = jnp.concatenate([res_in[k] for k in range(n_tp)], axis=1).astype(F32)
    mean = jnp.mean(combined * combined, axis=1, keepdims=True)
    out[...] = (kept + combined * lax.rsqrt(mean + EPS) * post_gain[...].astype(F32)).astype(BF16)


def local(
    stream_in, pre_gate, value_in, post_gate, conv_taps, out_weight, route_ids, route_weight,
    ffn_gain, post_gain, gate_proj, up_proj, down_proj,
):
    n_sp, n_tp = lax.axis_size("sp"), lax.axis_size("tp")
    own, features = stream_in.shape
    n_rows = pre_gate.shape[0]
    cap = 2 * own * route_ids.shape[1] // n_sp
    slots = n_sp * n_tp * cap
    vmem = pl.BlockSpec(memory_space=pltpu.VMEM)
    hbm = pl.BlockSpec(memory_space=pl.ANY)
    dma = pltpu.SemaphoreType.DMA
    chunks = CHUNKS
    return pl.pallas_call(
        functools.partial(kernel, (n_sp, n_tp, 4, cap)),
        out_shape=jax.ShapeDtypeStruct(stream_in.shape, BF16),
        in_specs=[vmem] * 10 + [hbm] * 3,
        out_specs=vmem,
        scratch_shapes=[
            pltpu.VMEM((16, 128), BF16),
            pltpu.VMEM((16, 128), BF16),
            pltpu.VMEM((n_tp, n_rows // 2, 128), BF16),
            pltpu.VMEM((n_tp, 64, 128), BF16),
            pltpu.VMEM((n_tp * 128, 256), BF16),
            pltpu.VMEM((n_tp, own, 128), BF16),
            pltpu.VMEM((n_tp, 8, n_rows // 2), F32),
            pltpu.VMEM((slots, n_rows), BF16),
            pltpu.VMEM((2 * n_rows, slots), BF16),
            pltpu.VMEM((n_rows, 128), F32),
            pltpu.VMEM((slots, 128), BF16),
            pltpu.VMEM((n_tp, slots, 128), BF16),
            pltpu.VMEM((n_tp, slots, 128), BF16),
            pltpu.VMEM((slots, 128), BF16),
            pltpu.VMEM((slots, 128), BF16),
            pltpu.VMEM((n_rows, 128), BF16),
            pltpu.VMEM((n_tp, own, 128), BF16),
            pltpu.VMEM((n_rows, 128), BF16),
            pltpu.VMEM((n_tp, own, 128), BF16),
            pltpu.VMEM((features, 256), BF16),
            pltpu.VMEM((features, 128), BF16),
            dma((3,)), dma((2,)), dma((8,)), dma((5,)), dma((8,)), dma((chunks,)),
            dma((len(OPS), 2, 4)), dma((len(OPS),)), dma((len(OPS),)), dma((chunks,)),
        ],
        compiler_params=pltpu.CompilerParams(
            collective_id=0, has_side_effects=True, vmem_limit_bytes=56 * 1024 * 1024
        ),
        cost_estimate=pl.CostEstimate(flops=4 * 10**9, bytes_accessed=3 * 10**6, transcendentals=0),
    )(
        stream_in, pre_gate, value_in, post_gate, conv_taps, out_weight, route_ids, route_weight,
        ffn_gain.reshape(1, features), post_gain.reshape(1, features),
        gate_proj, up_proj, down_proj,
    )


def solution(mesh):
    placed = (
        P(("sp", "tp"), None),
        P("sp", "tp"),
        P("sp", "tp"),
        P("sp", "tp"),
        P(None, "tp"),
        P("tp", None),
        P("sp", None),
        P("sp", None),
        P(),
        P(),
        P("sp", None, "tp"),
        P("sp", None, "tp"),
        P("sp", None, "tp"),
    )
    return jax.shard_map(
        local, mesh=mesh, in_specs=placed, out_specs=P(("sp", "tp"), None), check_vma=False
    )
```

```python
import functools

import jax
import jax.numpy as jnp
from jax import lax
from jax.experimental import pallas as pl
from jax.experimental.pallas import tpu as pltpu
from jax.sharding import PartitionSpec as P

MESH = pl.DeviceIdType.MESH
F32 = jnp.float32
BF16 = jnp.bfloat16
LIMIT = 7.0
SLOPE = 1.702
EPS = 1e-06
CHUNKS = 4
OPS = (("r", 0), ("r", 1), ("r", 2), ("r", 3), ("h", 0), ("h", 1), ("h", 2), ("h", 3))
STARTS = (0, 1, 2, 3, 5, 6, 7, 8)


def kernel(
    cfg,
    stream, pre, value, post, taps, weight, ids, route_w, ffn_gain, post_gain,
    gate_hbm, up_hbm, down_hbm,
    out,
    halo_src, halo_dst, mixed, w_in, w_diag, s_in, squares, picker, comb_w, aux, slot_cols,
    sent, rows, hidden, result, back, res_keep, res_in, comb_out, comb_in, w_gu, w_down,
    load_sem, halo_sem, small_send, small_recv, mix_recv, disp_recv, ring_recv, ring_pair,
    ring_send, back_recv,
):
    n_sp, n_tp, dim_x, cap = cfg
    dim_z, dim_y = n_sp // dim_x, n_tp // 2
    s, t = lax.axis_index("sp"), lax.axis_index("tp")
    sz, sx = s // dim_x, lax.rem(s, dim_x)
    y, core = t // 2, lax.rem(t, 2)
    n_rows = pre.shape[1]
    channels = pre.shape[0]
    top = ids.shape[0]
    own = n_rows // n_tp
    half = n_rows // 2
    block = own * cap * n_tp // own
    slots = block * n_sp
    per_chunk = n_sp // CHUNKS
    chunk = per_chunk * block

    def at_tp(step_y, other_core):
        to_core = 1 - core if other_core else core
        return lax.rem(y + step_y + dim_y, dim_y) * 2 + to_core

    def remote(src, dst, send, recv, tp=None, sp=None):
        target = {"tp": tp} if sp is None else {"sp": sp}
        return pltpu.make_async_remote_copy(
            src_ref=src, dst_ref=dst, send_sem=send, recv_sem=recv,
            device_id=target, device_id_type=MESH,
        )

    def drain(ref, sem):
        pltpu.make_async_copy(ref, ref, sem).wait()

    def z_step(p):
        place = p // dim_x
        return (place + 1) // 2 if place % 2 else (dim_z - place // 2) % dim_z

    loads = [
        pltpu.make_async_copy(gate_hbm.at[0], w_gu.at[:, pl.ds(0, 128)], load_sem.at[0]),
        pltpu.make_async_copy(up_hbm.at[0], w_gu.at[:, pl.ds(128, 128)], load_sem.at[1]),
        pltpu.make_async_copy(down_hbm.at[0], w_down, load_sem.at[2]),
    ]
    for load in loads:
        load.start()

    barrier = pltpu.get_barrier_semaphore()

    def greet_tp(step, carry):
        pl.semaphore_signal(
            barrier, inc=1, device_id={"tp": lax.rem(t + step, n_tp)}, device_id_type=MESH
        )
        return carry

    def greet_sp(step, carry):
        pl.semaphore_signal(
            barrier, inc=1, device_id={"sp": lax.rem(s + step, n_sp)}, device_id_type=MESH
        )
        return carry

    lax.fori_loop(1, n_tp, greet_tp, 0)
    lax.fori_loop(1, n_sp, greet_sp, 0)

    gated = (pre[...].astype(F32) * value[...].astype(F32)).astype(BF16).astype(F32)
    gates = jnp.transpose(jnp.concatenate([gated, post[...].astype(F32)], axis=0))
    halo_src[...] = gates[n_rows - 16 :, :].astype(BF16)

    pl.semaphore_wait(barrier, n_tp + n_sp - 2)

    halo = remote(
        halo_src, halo_dst, halo_sem.at[0], halo_sem.at[1], sp=lax.rem(s + 1, n_sp)
    )
    halo.start()

    tp_steps = [(d, o) for d in (4, 3, 5, 2, 6, 1, 7) for o in (False, True)] + [(0, True)]
    for step_y, other in tp_steps:
        to = at_tp(step_y, other)
        piece = pl.ds(pl.multiple_of(to * 128, 128), 128)
        remote(weight.at[:, piece], w_in.at[t], small_send.at[0], small_recv.at[0], tp=to).start()
    for step_y, other in tp_steps:
        to = at_tp(step_y, other)
        piece = pl.ds(pl.multiple_of(to * 128, 128), 128)
        remote(stream.at[:, piece], s_in.at[t], small_send.at[1], small_recv.at[1], tp=to).start()
    own_cols = pl.ds(pl.multiple_of(t * 128, 128), 128)
    w_in[t] = weight[:, own_cols]
    s_in[t] = stream[:, own_cols]

    aux[...] = jnp.zeros_like(aux)
    aux[0:top, :] = ids[...].astype(F32)
    aux[top : 2 * top, :] = route_w[...]
    by_row = jnp.transpose(aux[...])
    id_cols = [by_row[:, k : k + 1] for k in range(top)]
    amounts = [by_row[:, top + k : top + k + 1] for k in range(top)]
    lane = lax.broadcasted_iota(jnp.int32, (n_rows, 128), 1)
    lane_f = lane.astype(F32)
    named = jnp.zeros((n_rows, 128), F32)
    for k in range(top):
        named = named + jnp.where(id_cols[k] == lane_f, 1.0, 0.0)
    row_a = lax.broadcasted_iota(jnp.int32, (n_rows, n_rows), 0)
    row_b = lax.broadcasted_iota(jnp.int32, (n_rows, n_rows), 1)
    earlier = jnp.where((row_a > row_b) & (row_a // own == row_b // own), 1.0, 0.0).astype(BF16)
    rank = jnp.dot(earlier, named.astype(BF16), preferred_element_type=F32)
    dz = lax.rem(sz - lane // dim_x + 32 * dim_z, dim_z)
    dx = lax.rem(sx - lax.rem(lane, dim_x) + 32 * dim_x, dim_x)
    z_place = jnp.where(dz * 2 <= dim_z, jnp.maximum(2 * dz - 1, 0), 2 * (dim_z - dz))
    at_row = lax.broadcasted_iota(jnp.int32, (n_rows, 128), 0)
    slot_of = ((z_place * dim_x + dx) * block + (at_row // own) * cap).astype(F32) + rank
    places = [
        jnp.sum(jnp.where(id_cols[k] == lane_f, slot_of, 0.0), axis=1, keepdims=True)
        for k in range(top)
    ]
    columns = jnp.zeros((n_rows, 128), F32)
    for k in range(top):
        columns = jnp.where(lane == k, places[k], columns)
        columns = jnp.where(lane == top + k, amounts[k], columns)
    slot_cols[...] = columns
    slot_rows = jnp.transpose(columns)
    w_diag[...] = jnp.zeros_like(w_diag)

    wide, second = gates[:, :channels], gates[:, channels:]
    tap = taps[...].astype(F32)
    row_no = lax.broadcasted_iota(jnp.int32, wide.shape, 0)
    shift_1, shift_2 = pltpu.roll(wide, 1, 0), pltpu.roll(wide, 2, 0)
    halo.wait_recv()
    rim = halo_dst[...].astype(F32)[:, :channels]
    rim = jnp.where(s > 0, rim, 0.0)
    last, before_last = rim[15:16, :], rim[14:15, :]
    shift_1 = jnp.where(row_no == 0, last, shift_1)
    shift_2 = jnp.where(row_no == 0, before_last, jnp.where(row_no == 1, last, shift_2))
    convolved = tap[0:1] * shift_2
    convolved = convolved + tap[1:2] * shift_1
    convolved = convolved + tap[2:3] * wide
    mixer = second * convolved
    mixed[t] = jnp.concatenate([mixer[:half], mixer[half:]], axis=1).astype(BF16)

    steps = (4, 3, 5, 2, 6, 1, 7)
    for step_y in steps:
        remote(
            mixed.at[t], mixed.at[t], small_send.at[2], mix_recv.at[step_y], tp=at_tp(step_y, False)
        ).start()
    partner = at_tp(0, True)
    remote(mixed.at[t], mixed.at[t], small_send.at[2], mix_recv.at[0], tp=partner).start()

    def fill_picker(part, carry):
        first = pl.multiple_of(part * 256, 256)
        number = lax.broadcasted_iota(jnp.int32, (256, n_rows), 0) + part * 256
        number = number.astype(F32)
        hit = number == slot_rows[0:1, :]
        for k in range(1, top):
            hit = hit | (number == slot_rows[k : k + 1, :])
        picker[pl.ds(first, 256), :] = jnp.where(hit, 1.0, 0.0).astype(BF16)
        return carry

    lax.fori_loop(0, slots // 256, fill_picker, 0)

    drain(w_in.at[pl.ds(0, n_tp - 1)], small_recv.at[0])
    for k in range(n_tp):
        piece = w_in[k]
        w_diag[pl.ds(k * 128, 64), pl.ds(0, 128)] = piece
        w_diag[pl.ds(k * 128 + 64, 64), pl.ds(128, 128)] = piece
    for step_y in steps:
        arrived = mixed.at[at_tp(-step_y, False)]
        drain(arrived, mix_recv.at[step_y])
        remote(arrived, arrived, small_send.at[2], mix_recv.at[0], tp=partner).start()
    drain(s_in.at[pl.ds(0, n_tp - 1)], small_recv.at[1])
    drain(mixed.at[pl.ds(0, dim_y)], mix_recv.at[0])
    stacked = jnp.concatenate([mixed[k] for k in range(n_tp)], axis=1)
    projected = jnp.dot(stacked, w_diag[...], preferred_element_type=F32)
    projected = jnp.concatenate([projected[:, :128], projected[:, 128:]], axis=0)
    residual = (s_in[...].reshape(n_rows, 128).astype(F32) + projected).astype(BF16)
    res_keep[...] = residual
    res = residual.astype(F32)

    sums = jnp.sum(res * res, axis=1, keepdims=True)
    across = jnp.transpose(jnp.broadcast_to(sums, (n_rows, 128)))
    first_row = lax.broadcasted_iota(jnp.int32, (8, half), 0) == 0
    squares[t] = jnp.where(first_row, across[0:8, :half], across[0:8, half:])
    for step_y, other in tp_steps:
        remote(
            squares.at[t], squares.at[t], small_send.at[3], small_recv.at[2],
            tp=at_tp(step_y, other),
        ).start()
    drain(squares.at[pl.ds(0, n_tp - 1)], small_recv.at[2])
    total = squares[0]
    for k in range(1, n_tp):
        total = total + squares[k]
    scale = lax.rsqrt(total / (n_tp * 128) + EPS)
    scale = jnp.concatenate(
        [jnp.transpose(jnp.broadcast_to(scale[k : k + 1, :], (half, half))) for k in range(2)], axis=0
    )
    gains = ffn_gain[...].astype(F32).reshape(n_tp, 128)
    gain_no = lax.broadcasted_iota(jnp.int32, (n_tp, 128), 0)
    gain = jnp.sum(jnp.where(gain_no == t, gains, 0.0), axis=0, keepdims=True)
    normed = (res * scale * gain).astype(BF16)

    for part in range(CHUNKS):
        span = pl.ds(part * chunk, chunk)
        picked = jnp.dot(picker[span, :], normed, preferred_element_type=F32).astype(BF16)
        sent[span, :] = picked
        if part == 0:
            rows[t, pl.ds(0, block), :] = picked[:block]
        for p in range(max(1, part * per_chunk), (part + 1) * per_chunk):
            to_z = lax.rem(sz - z_step(p) + dim_z, dim_z)
            to_x = lax.rem(sx - p % dim_x + dim_x, dim_x)
            place = pl.ds(p * block, block)
            remote(
                sent.at[place, :], rows.at[t, place, :], small_send.at[5], disp_recv.at[part],
                sp=to_z * dim_x + to_x,
            ).start()

    for step_y, other in tp_steps:
        to = at_tp(step_y, other)
        remote(
            res_keep.at[pl.ds(pl.multiple_of(to * own, own), own), :], res_in.at[t],
            small_send.at[4], small_recv.at[3], tp=to,
        ).start()
    res_in[t] = res_keep[pl.ds(pl.multiple_of(t * own, own), own), :]

    def fill_weights(part, carry):
        first = pl.multiple_of(part * 256, 256)
        number = lax.broadcasted_iota(jnp.int32, (n_rows, 256), 1) + part * 256
        number = number.astype(F32)
        columns = slot_cols[...]
        summed = jnp.zeros((n_rows, 256), F32)
        for k in range(top):
            summed = summed + jnp.where(
                number == columns[:, k : k + 1], columns[:, top + k : top + k + 1], 0.0
            )
        high = summed.astype(BF16)
        comb_w[pl.ds(0, n_rows), pl.ds(first, 256)] = high
        comb_w[pl.ds(n_rows, n_rows), pl.ds(first, 256)] = (summed - high.astype(F32)).astype(BF16)
        return carry

    def weights(i, part):
        lax.fori_loop(0, slots // 256, fill_weights, 0)

    for load in loads:
        load.wait()

    lower, upper = chunk // 2, chunk - chunk // 2

    def units(i, part):
        span = pl.ds(i * chunk + part * lower, lower)
        held = jnp.concatenate([rows[k, span, :] for k in range(n_tp)], axis=1)
        both = jnp.dot(held, w_gu[...], preferred_element_type=F32)
        gate = jnp.minimum(both[:, :128], LIMIT)
        up = jnp.clip(both[:, 128:], -LIMIT, LIMIT)
        hidden[t, span, :] = ((up + 1.0) * (gate * jax.nn.sigmoid(SLOPE * gate))).astype(BF16)

    def outputs(i, part):
        span = pl.ds(i * chunk + part * lower, lower)
        held = jnp.concatenate([hidden[k, span, :] for k in range(n_tp)], axis=1)
        result[span, :] = jnp.dot(held, w_down[...], preferred_element_type=F32).astype(BF16)

    def send_back(i):
        for p in range(i * per_chunk, (i + 1) * per_chunk):
            place = pl.ds(p * block, block)
            if p == 0:
                back[place, :] = result[place, :]
                continue
            to_z = lax.rem(sz + z_step(p), dim_z)
            to_x = lax.rem(sx + p % dim_x, dim_x)
            remote(
                result.at[place, :], back.at[place, :], small_send.at[6], back_recv.at[i],
                sp=to_z * dim_x + to_x,
            ).start()

    right, left = at_tp(1, False), at_tp(-1, False)

    def ring_step(j, d):
        kind, i = OPS[j]
        held = rows if kind == "r" else hidden
        full = pl.ds(i * chunk, chunk)
        first = pl.ds(i * chunk, lower)
        second = pl.ds(i * chunk + lower, upper)

        def pass_on(origin, span, to, sem):
            piece = held.at[origin, span, :]
            remote(piece, piece, ring_send.at[j], sem, tp=to).start()

        if d == 0:
            if kind == "r":
                taken = (per_chunk - (1 if i == 0 else 0)) * block
                drain(sent.at[pl.ds(0, taken), :], disp_recv.at[i])
            pass_on(t, full, right, ring_recv.at[j, 0, 0])
            pass_on(t, full, left, ring_recv.at[j, 1, 0])
            pass_on(t, full, partner, ring_pair.at[j])
            return
        for way, sign, ahead, end in ((0, -1, right, first), (1, 1, left, second)):
            origin = at_tp(sign * d, False)
            span = full if d < 4 else end
            drain(held.at[origin, span, :], ring_recv.at[j, way, d - 1])
            if d < 4:
                pass_on(origin, full if d < 3 else end, ahead, ring_recv.at[j, way, d])
            pass_on(origin, span, partner, ring_pair.at[j])
        if d == 4:
            drain(held.at[pl.ds(0, dim_y), full, :], ring_pair.at[j])

    work = {2: [(weights, 0, 0)]}
    for i in range(CHUNKS):
        work.setdefault(4 + i, []).extend([(units, i, 0), (units, i, 1)])
        work.setdefault(9 + i, []).extend([(outputs, i, 0), (outputs, i, 1)])
    for slot in range(STARTS[-1] + 5):
        for j in range(len(OPS)):
            d = slot - STARTS[j]
            if 0 <= d <= 4:
                ring_step(j, d)
        for task, i, part in work.get(slot, ()):
            task(i, part)
            if task is outputs and part == 1:
                send_back(i)

    summed = jnp.zeros((2 * n_rows, 128), F32)
    for i in range(CHUNKS):
        taken = (per_chunk - (1 if i == 0 else 0)) * block
        drain(back.at[pl.ds(0, taken), :], back_recv.at[i])
        span = pl.ds(i * chunk, chunk)
        summed = summed + jnp.dot(comb_w[:, span], back[span, :], preferred_element_type=F32)
    comb_out[...] = (summed[:n_rows] + summed[n_rows:]).astype(BF16)
    for step_y, other in tp_steps:
        to = at_tp(step_y, other)
        remote(
            comb_out.at[pl.ds(pl.multiple_of(to * own, own), own), :], comb_in.at[t],
            small_send.at[7], small_recv.at[4], tp=to,
        ).start()
    comb_in[t] = comb_out[pl.ds(pl.multiple_of(t * own, own), own), :]

    halo.wait_send()
    drain(w_in.at[pl.ds(0, n_tp - 1)], small_send.at[0])
    drain(s_in.at[pl.ds(0, n_tp - 1)], small_send.at[1])
    drain(mixed.at[pl.ds(0, 2 * dim_y - 1)], small_send.at[2])
    drain(squares.at[pl.ds(0, n_tp - 1)], small_send.at[3])
    drain(res_in.at[pl.ds(0, n_tp - 1)], small_send.at[4])
    drain(sent.at[pl.ds(0, slots - block), :], small_send.at[5])
    drain(result.at[pl.ds(0, slots - block), :], small_send.at[6])
    for j in range(len(OPS)):
        drain(rows.at[pl.ds(0, 15), pl.ds(0, chunk), :], ring_send.at[j])

    drain(res_in.at[pl.ds(0, n_tp - 1)], small_recv.at[3])
    drain(comb_in.at[pl.ds(0, n_tp - 1)], small_recv.at[4])
    drain(comb_in.at[pl.ds(0, n_tp - 1)], small_send.at[7])
    combined = jnp.concatenate([comb_in[k] for k in range(n_tp)], axis=1).astype(F32)
    kept = jnp.concatenate([res_in[k] for k in range(n_tp)], axis=1).astype(F32)
    mean = jnp.mean(combined * combined, axis=1, keepdims=True)
    out[...] = (kept + combined * lax.rsqrt(mean + EPS) * post_gain[...].astype(F32)[None, :]).astype(BF16)


def local(
    stream_in, pre_gate, value_in, post_gate, conv_taps, out_weight, route_ids, route_weight,
    ffn_gain, post_gain, gate_proj, up_proj, down_proj,
):
    n_sp, n_tp = lax.axis_size("sp"), lax.axis_size("tp")
    own, features = stream_in.shape
    n_rows = pre_gate.shape[0]
    cap = 2 * own * route_ids.shape[1] // n_sp
    slots = n_sp * n_tp * cap
    vmem = pl.BlockSpec(memory_space=pltpu.VMEM)
    hbm = pl.BlockSpec(memory_space=pl.ANY)
    dma = pltpu.SemaphoreType.DMA
    chunks = CHUNKS
    return pl.pallas_call(
        functools.partial(kernel, (n_sp, n_tp, 4, cap)),
        out_shape=jax.ShapeDtypeStruct(stream_in.shape, BF16),
        in_specs=[vmem] * 10 + [hbm] * 3,
        out_specs=vmem,
        scratch_shapes=[
            pltpu.VMEM((16, 128), BF16),
            pltpu.VMEM((16, 128), BF16),
            pltpu.VMEM((n_tp, n_rows // 2, 128), BF16),
            pltpu.VMEM((n_tp, 64, 128), BF16),
            pltpu.VMEM((n_tp * 128, 256), BF16),
            pltpu.VMEM((n_tp, own, 128), BF16),
            pltpu.VMEM((n_tp, 8, n_rows // 2), F32),
            pltpu.VMEM((slots, n_rows), BF16),
            pltpu.VMEM((2 * n_rows, slots), BF16),
            pltpu.VMEM((128, n_rows), F32),
            pltpu.VMEM((n_rows, 128), F32),
            pltpu.VMEM((slots, 128), BF16),
            pltpu.VMEM((n_tp, slots, 128), BF16),
            pltpu.VMEM((n_tp, slots, 128), BF16),
            pltpu.VMEM((slots, 128), BF16),
            pltpu.VMEM((slots, 128), BF16),
            pltpu.VMEM((n_rows, 128), BF16),
            pltpu.VMEM((n_tp, own, 128), BF16),
            pltpu.VMEM((n_rows, 128), BF16),
            pltpu.VMEM((n_tp, own, 128), BF16),
            pltpu.VMEM((features, 256), BF16),
            pltpu.VMEM((features, 128), BF16),
            dma((3,)), dma((2,)), dma((8,)), dma((5,)), dma((8,)), dma((chunks,)),
            dma((len(OPS), 2, 4)), dma((len(OPS),)), dma((len(OPS),)), dma((chunks,)),
        ],
        compiler_params=pltpu.CompilerParams(
            collective_id=0, has_side_effects=True, vmem_limit_bytes=56 * 1024 * 1024
        ),
        cost_estimate=pl.CostEstimate(flops=4 * 10**9, bytes_accessed=3 * 10**6, transcendentals=0),
    )(
        stream_in, pre_gate.T, value_in.T, post_gate.T, conv_taps, out_weight,
        route_ids.T, route_weight.T,
        ffn_gain, post_gain,
        gate_proj, up_proj, down_proj,
    )


def solution(mesh):
    placed = (
        P(("sp", "tp"), None),
        P("sp", "tp"),
        P("sp", "tp"),
        P("sp", "tp"),
        P(None, "tp"),
        P("tp", None),
        P("sp", None),
        P("sp", None),
        P(),
        P(),
        P("sp", None, "tp"),
        P("sp", None, "tp"),
        P("sp", None, "tp"),
    )
    return jax.shard_map(
        local, mesh=mesh, in_specs=placed, out_specs=P(("sp", "tp"), None), check_vma=False
    )
```

```python
import functools

import jax
import jax.numpy as jnp
from jax import lax
from jax.experimental import pallas as pl
from jax.experimental.pallas import tpu as pltpu
from jax.sharding import PartitionSpec as P

MESH = pl.DeviceIdType.MESH
F32 = jnp.float32
BF16 = jnp.bfloat16
LIMIT = 7.0
SLOPE = 1.702
EPS = 1e-06
OFFSETS = (0, 1, -1, 2, -2, 3, -3, 4)
AT = {offset: place for place, offset in enumerate(OFFSETS)}
NEAR, FAR = (0, 1, 2, 3, 4), (5, 6, 7)
EARLY, LATE = (0, 1, 2), (3, 4)
FIRST_SLICES = 3
OPS = (('g', 0, 0), ('r', 5, 2), ('r', 6, 3), ('r', 7, 4), ('h', 5, 7), ('h', 6, 8), ('h', 7, 9), ('h', 0, 10), ('h', 1, 11), ('h', 2, 12), ('h', 3, 13), ('h', 4, 14))
WORK = {1: [('pick', 0)], 3: [('weights', 0)], 4: [('pick', 1)], 6: [('units', 5)], 7: [('units', 6)], 8: [('units', 7), ('across', 0)], 9: [('units', 0), ('across', 1)], 10: [('units', 1), ('across', 2)], 11: [('units', 2), ('across', 3)], 12: [('units', 3), ('across', 4)], 13: [('units', 4)]}


def kernel(
    cfg,
    stream, pre, value, post, taps, weight, ids, route_w, ffn_gain, post_gain,
    gate_hbm, up_hbm, down_hbm,
    out,
    halo_src, halo_dst, mixed, w_in, w_diag, s_in, squares, picker, comb_w, aux, slot_cols,
    norms, far_out, near_out, rows, hidden, result, back, res_keep, res_in, comb_out, comb_in, w_gu, w_down,
    load_sem, halo_sem, small_send, small_recv, mix_recv, far_recv, near_recv, near_pair,
    ring_recv, ring_pair, ring_send, back_recv,
):
    n_sp, n_tp, dim_x, cap = cfg
    dim_z, dim_y = n_sp // dim_x, n_tp // 2
    s, t = lax.axis_index("sp"), lax.axis_index("tp")
    sz, sx = s // dim_x, lax.rem(s, dim_x)
    y, core = t // 2, lax.rem(t, 2)
    n_rows = pre.shape[1]
    channels = pre.shape[0]
    top = ids.shape[0]
    own = n_rows // n_tp
    half = n_rows // 2
    block = own * cap * n_tp // own
    slots = block * n_sp
    zone = dim_x * block

    def at_tp(step_y, other_core):
        to_core = 1 - core if other_core else core
        return lax.rem(y + step_y + dim_y, dim_y) * 2 + to_core

    def remote(src, dst, send, recv, tp=None, sp=None):
        target = {"tp": tp} if sp is None else {"sp": sp}
        return pltpu.make_async_remote_copy(
            src_ref=src, dst_ref=dst, send_sem=send, recv_sem=recv,
            device_id=target, device_id_type=MESH,
        )

    def drain(ref, sem):
        pltpu.make_async_copy(ref, ref, sem).wait()

    def z_step(p):
        place = p // dim_x
        return (place + 1) // 2 if place % 2 else (dim_z - place // 2) % dim_z

    for core_no in range(2):
        for place, offset in enumerate(OFFSETS):
            origin = pl.ds(pl.multiple_of(at_tp(offset, core_no == 1) * 128, 128), 128)
            here = pl.ds((core_no * dim_y + place) * 128, 128)
            pltpu.make_async_copy(
                gate_hbm.at[0, origin, :], w_gu.at[here, pl.ds(0, 128)], load_sem.at[0]
            ).start()
            pltpu.make_async_copy(
                up_hbm.at[0, origin, :], w_gu.at[here, pl.ds(128, 128)], load_sem.at[1]
            ).start()
            pltpu.make_async_copy(
                down_hbm.at[0, origin, :], w_down.at[here, :], load_sem.at[2]
            ).start()

    barrier = pltpu.get_barrier_semaphore()

    def greet_tp(step, carry):
        pl.semaphore_signal(
            barrier, inc=1, device_id={"tp": lax.rem(t + step, n_tp)}, device_id_type=MESH
        )
        return carry

    def greet_sp(step, carry):
        pl.semaphore_signal(
            barrier, inc=1, device_id={"sp": lax.rem(s + step, n_sp)}, device_id_type=MESH
        )
        return carry

    lax.fori_loop(1, n_tp, greet_tp, 0)
    lax.fori_loop(1, n_sp, greet_sp, 0)

    gated = (pre[...].astype(F32) * value[...].astype(F32)).astype(BF16).astype(F32)
    gates = jnp.transpose(jnp.concatenate([gated, post[...].astype(F32)], axis=0))
    halo_src[...] = gates[n_rows - 16 :, :].astype(BF16)

    pl.semaphore_wait(barrier, n_tp + n_sp - 2)

    halo = remote(
        halo_src, halo_dst, halo_sem.at[0], halo_sem.at[1], sp=lax.rem(s + 1, n_sp)
    )
    halo.start()

    share = weight.shape[0] // dim_x
    quarter = pl.ds(pl.multiple_of(sx * share, share), share)
    tp_steps = [(d, o) for d in (4, 3, 5, 2, 6, 1, 7) for o in (False, True)] + [(0, True)]
    for step_y, other in tp_steps:
        to = at_tp(step_y, other)
        piece = pl.ds(pl.multiple_of(to * 128, 128), 128)
        remote(
            weight.at[quarter, piece], w_in.at[sx, t], small_send.at[0], small_recv.at[0], tp=to
        ).start()
    for step_y, other in tp_steps:
        to = at_tp(step_y, other)
        piece = pl.ds(pl.multiple_of(to * 128, 128), 128)
        remote(stream.at[:, piece], s_in.at[t], small_send.at[1], small_recv.at[1], tp=to).start()
    own_cols = pl.ds(pl.multiple_of(t * 128, 128), 128)
    w_in[sx, t] = weight[quarter, own_cols]
    s_in[t] = stream[:, own_cols]

    aux[...] = jnp.zeros_like(aux)
    aux[0:top, :] = ids[...].astype(F32)
    aux[top : 2 * top, :] = route_w[...]
    by_row = jnp.transpose(aux[...])
    id_cols = [by_row[:, k : k + 1] for k in range(top)]
    amounts = [by_row[:, top + k : top + k + 1] for k in range(top)]
    lane = lax.broadcasted_iota(jnp.int32, (n_rows, 128), 1)
    lane_f = lane.astype(F32)
    named = jnp.zeros((n_rows, 128), F32)
    for k in range(top):
        named = named + jnp.where(id_cols[k] == lane_f, 1.0, 0.0)
    row_a = lax.broadcasted_iota(jnp.int32, (n_rows, n_rows), 0)
    row_b = lax.broadcasted_iota(jnp.int32, (n_rows, n_rows), 1)
    earlier = jnp.where((row_a > row_b) & (row_a // own == row_b // own), 1.0, 0.0).astype(BF16)
    rank = jnp.dot(earlier, named.astype(BF16), preferred_element_type=F32)
    dz = lax.rem(sz - lane // dim_x + 32 * dim_z, dim_z)
    dx = lax.rem(sx - lax.rem(lane, dim_x) + 32 * dim_x, dim_x)
    z_place = jnp.where(dz * 2 <= dim_z, jnp.maximum(2 * dz - 1, 0), 2 * (dim_z - dz))
    at_row = lax.broadcasted_iota(jnp.int32, (n_rows, 128), 0)
    slot_of = ((z_place * dim_x + dx) * block + (at_row // own) * cap).astype(F32) + rank
    places = [
        jnp.sum(jnp.where(id_cols[k] == lane_f, slot_of, 0.0), axis=1, keepdims=True)
        for k in range(top)
    ]
    columns = jnp.zeros((n_rows, 128), F32)
    for k in range(top):
        columns = jnp.where(lane == k, places[k], columns)
        columns = jnp.where(lane == top + k, amounts[k], columns)
    slot_cols[...] = columns
    slot_rows = jnp.transpose(columns)
    w_diag[...] = jnp.zeros_like(w_diag)

    wide, second = gates[:, :channels], gates[:, channels:]
    tap = taps[...].astype(F32)
    row_no = lax.broadcasted_iota(jnp.int32, wide.shape, 0)
    shift_1, shift_2 = pltpu.roll(wide, 1, 0), pltpu.roll(wide, 2, 0)
    halo.wait_recv()
    rim = halo_dst[...].astype(F32)[:, :channels]
    rim = jnp.where(s > 0, rim, 0.0)
    last, before_last = rim[15:16, :], rim[14:15, :]
    shift_1 = jnp.where(row_no == 0, last, shift_1)
    shift_2 = jnp.where(row_no == 0, before_last, jnp.where(row_no == 1, last, shift_2))
    convolved = tap[0:1] * shift_2
    convolved = convolved + tap[1:2] * shift_1
    convolved = convolved + tap[2:3] * wide
    mixer = second * convolved
    mixed[t] = jnp.concatenate([mixer[:half], mixer[half:]], axis=1).astype(BF16)

    steps = (4, 3, 5, 2, 6, 1, 7)
    for step_y in steps:
        remote(
            mixed.at[t], mixed.at[t], small_send.at[2], mix_recv.at[step_y], tp=at_tp(step_y, False)
        ).start()
    partner = at_tp(0, True)
    remote(mixed.at[t], mixed.at[t], small_send.at[2], mix_recv.at[0], tp=partner).start()
    drain(w_in.at[sx, pl.ds(0, n_tp - 1)], small_recv.at[0])
    for step_x in (2, 1, 3):
        remote(
            w_in.at[sx], w_in.at[sx], small_send.at[10], small_recv.at[5],
            sp=sz * dim_x + lax.rem(sx + step_x, dim_x),
        ).start()

    def fill_picker(part, carry):
        first = pl.multiple_of(part * 256, 256)
        number = lax.broadcasted_iota(jnp.int32, (256, n_rows), 0) + part * 256
        number = number.astype(F32)
        hit = number == slot_rows[0:1, :]
        for k in range(1, top):
            hit = hit | (number == slot_rows[k : k + 1, :])
        picker[pl.ds(first, 256), :] = jnp.where(hit, 1.0, 0.0).astype(BF16)
        return carry

    lax.fori_loop(0, slots // 256, fill_picker, 0)

    drain(w_in.at[pl.ds(0, dim_x - 1)], small_recv.at[5])
    for k in range(n_tp):
        piece = jnp.concatenate([w_in[x, k] for x in range(dim_x)], axis=0)
        w_diag[pl.ds(k * 128, 64), pl.ds(0, 128)] = piece
        w_diag[pl.ds(k * 128 + 64, 64), pl.ds(128, 128)] = piece
    for step_y in steps:
        arrived = mixed.at[at_tp(-step_y, False)]
        drain(arrived, mix_recv.at[step_y])
        remote(arrived, arrived, small_send.at[2], mix_recv.at[0], tp=partner).start()
    drain(s_in.at[pl.ds(0, n_tp - 1)], small_recv.at[1])
    drain(mixed.at[pl.ds(0, dim_y)], mix_recv.at[0])
    stacked = jnp.concatenate([mixed[k] for k in range(n_tp)], axis=1)
    projected = jnp.dot(stacked, w_diag[...], preferred_element_type=F32)
    projected = jnp.concatenate([projected[:, :128], projected[:, 128:]], axis=0)
    residual = (s_in[...].reshape(n_rows, 128).astype(F32) + projected).astype(BF16)
    res_keep[...] = residual
    res = residual.astype(F32)

    sums = jnp.sum(res * res, axis=1, keepdims=True)
    across = jnp.transpose(jnp.broadcast_to(sums, (n_rows, 128)))
    first_row = lax.broadcasted_iota(jnp.int32, (8, half), 0) == 0
    squares[t] = jnp.where(first_row, across[0:8, :half], across[0:8, half:])
    for step_y, other in tp_steps:
        remote(
            squares.at[t], squares.at[t], small_send.at[3], small_recv.at[2],
            tp=at_tp(step_y, other),
        ).start()
    drain(squares.at[pl.ds(0, n_tp - 1)], small_recv.at[2])
    total = squares[0]
    for k in range(1, n_tp):
        total = total + squares[k]
    scale = lax.rsqrt(total / (n_tp * 128) + EPS)
    scale = jnp.concatenate(
        [jnp.transpose(jnp.broadcast_to(scale[k : k + 1, :], (half, half))) for k in range(2)], axis=0
    )
    gains = ffn_gain[...].astype(F32).reshape(n_tp, 128)
    gain_no = lax.broadcasted_iota(jnp.int32, (n_tp, 128), 0)
    gain = jnp.sum(jnp.where(gain_no == t, gains, 0.0), axis=0, keepdims=True)
    normed = (res * scale * gain).astype(BF16)

    norms[0] = normed

    right, left = at_tp(1, False), at_tp(-1, False)
    lower, upper = zone // 2, zone - zone // 2

    def ring_step(j, d):
        kind, z, _ = OPS[j]
        base = 0 if kind == "g" else z * zone

        def part(place, span, core_no=0):
            first, size = span
            span = pl.ds(base + first, size)
            if kind == "g":
                return norms.at[place, span, :]
            return (rows if kind == "r" else hidden).at[core_no, place, span, :]

        def pass_on(origin, shifted, span, to, sem):
            remote(part(origin, span), part(shifted, span), ring_send.at[j], sem, tp=to).start()

        def cross(place, span):
            if kind != "g":
                remote(
                    part(place, span), part(place, span, 1), ring_send.at[j], ring_pair.at[j],
                    tp=partner,
                ).start()

        full, first, second = (0, zone), (0, lower), (lower, upper)
        if d == 0:
            if kind == "r":
                drain(part(0, full), far_recv.at[z - FAR[0]])
            pass_on(AT[0], AT[-1], full, right, ring_recv.at[j, 0, 0])
            pass_on(AT[0], AT[1], full, left, ring_recv.at[j, 1, 0])
            cross(AT[0], full)
            return
        for way, sign, ahead, end in ((0, -1, right, first), (1, 1, left, second)):
            origin = AT[sign * d] if d < 4 else AT[4]
            span = full if d < 4 else end
            drain(part(origin, span), ring_recv.at[j, way, d - 1])
            if d < 4:
                shifted = AT[sign * (d + 1)] if d < 3 else AT[4]
                pass_on(origin, shifted, full if d < 3 else end, ahead, ring_recv.at[j, way, d])
            cross(origin, span)
        if d == 4 and kind != "g":
            drain(
                (rows if kind == "r" else hidden).at[1, :, pl.ds(base, zone), :], ring_pair.at[j]
            )

    ring_step(0, 0)

    def expert_of(p):
        to_z = lax.rem(sz - z_step(p) + dim_z, dim_z)
        return to_z * dim_x + lax.rem(sx - p % dim_x + dim_x, dim_x)

    for z in FAR:
        base = (z - FAR[0]) * zone
        far_out[pl.ds(base, zone), :] = jnp.dot(
            picker[pl.ds(z * zone, zone), :], normed, preferred_element_type=F32
        ).astype(BF16)
        for x in range(dim_x):
            p = z * dim_x + x
            remote(
                far_out.at[pl.ds(base + x * block, block), :],
                rows.at[0, 0, pl.ds(p * block, block), :],
                small_send.at[5], far_recv.at[z - FAR[0]], sp=expert_of(p),
            ).start()

    def pick_zone(z, first, last):
        span = pl.ds(z * zone, zone)
        wide_rows = jnp.concatenate([norms[k] for k in range(first, last)], axis=1)
        picked = jnp.dot(picker[span, :], wide_rows, preferred_element_type=F32).astype(BF16)
        for k in range(first, last):
            piece = picked[:, (k - first) * 128 : (k - first + 1) * 128]
            near_out[k, span, :] = piece
            if z == 0:
                rows[0, k, pl.ds(0, block), :] = piece[:block]
        for x in range(dim_x):
            p = z * dim_x + x
            if p == 0:
                continue
            place = pl.ds(p * block, block)
            remote(
                near_out.at[pl.ds(first, last - first), place, :],
                rows.at[0, pl.ds(first, last - first), place, :],
                small_send.at[6], near_recv.at[z], sp=expert_of(p),
            ).start()

    def pick(batch):
        if batch == 0:
            for z in EARLY:
                pick_zone(z, 0, FIRST_SLICES)
            return
        for z in EARLY:
            pick_zone(z, FIRST_SLICES, dim_y)
        for z in LATE:
            pick_zone(z, 0, dim_y)

    def across(z):
        own_x = 1 if z == 0 else 0
        taken = pl.ds(z * zone, zone - own_x * block)
        drain(rows.at[0, :, taken, :], near_recv.at[z])
        span = pl.ds(z * zone, zone)
        remote(
            rows.at[0, :, span, :], rows.at[1, :, span, :], small_send.at[8], near_pair.at[z],
            tp=partner,
        ).start()

    for step_y, other in tp_steps:
        to = at_tp(step_y, other)
        remote(
            res_keep.at[pl.ds(pl.multiple_of(to * own, own), own), :], res_in.at[t],
            small_send.at[4], small_recv.at[3], tp=to,
        ).start()
    res_in[t] = res_keep[pl.ds(pl.multiple_of(t * own, own), own), :]

    def fill_weights(part, carry):
        first = pl.multiple_of(part * 256, 256)
        number = lax.broadcasted_iota(jnp.int32, (n_rows, 256), 1) + part * 256
        number = number.astype(F32)
        columns = slot_cols[...]
        summed = jnp.zeros((n_rows, 256), F32)
        for k in range(top):
            summed = summed + jnp.where(
                number == columns[:, k : k + 1], columns[:, top + k : top + k + 1], 0.0
            )
        high = summed.astype(BF16)
        comb_w[pl.ds(0, n_rows), pl.ds(first, 256)] = high
        comb_w[pl.ds(n_rows, n_rows), pl.ds(first, 256)] = (summed - high.astype(F32)).astype(BF16)
        return carry

    def weights(z):
        lax.fori_loop(0, slots // 256, fill_weights, 0)

    drain(w_gu.at[:, pl.ds(0, 128)], load_sem.at[0])
    drain(w_gu.at[:, pl.ds(128, 128)], load_sem.at[1])
    drain(w_down, load_sem.at[2])

    def stacked_rows(held, z):
        span = pl.ds(z * zone, zone)
        return jnp.concatenate(
            [held[core_no, k, span, :] for core_no in range(2) for k in range(dim_y)], axis=1
        )

    def units(z):
        span = pl.ds(z * zone, zone)
        if z in NEAR:
            drain(rows.at[1, :, span, :], near_pair.at[z])
        both = jnp.dot(stacked_rows(rows, z), w_gu[...], preferred_element_type=F32)
        gate = jnp.minimum(both[:, :128], LIMIT)
        up = jnp.clip(both[:, 128:], -LIMIT, LIMIT)
        hidden[0, 0, span, :] = ((up + 1.0) * (gate * jax.nn.sigmoid(SLOPE * gate))).astype(BF16)

    def outputs(z):
        span = pl.ds(z * zone, zone)
        done = jnp.dot(stacked_rows(hidden, z), w_down[...], preferred_element_type=F32)
        result[span, :] = done.astype(BF16)
        for x in range(dim_x):
            p = z * dim_x + x
            place = pl.ds(p * block, block)
            if p == 0:
                back[place, :] = result[place, :]
                continue
            to_z = lax.rem(sz + z_step(p), dim_z)
            to_x = lax.rem(sx + x, dim_x)
            remote(
                result.at[place, :], back.at[place, :], small_send.at[9], back_recv.at[z],
                sp=to_z * dim_x + to_x,
            ).start()

    tasks = dict(pick=pick, weights=weights, across=across, units=units)
    for slot in range(max(op[2] for op in OPS) + 5):
        finished = []
        for j, (kind, z, start) in enumerate(OPS):
            d = slot - start
            if 0 <= d <= 4 and (j, d) != (0, 0):
                ring_step(j, d)
                if d == 4 and kind == "h":
                    finished.append(z)
        for name, z in WORK.get(slot, ()):
            tasks[name](z)
        for z in finished:
            outputs(z)

    summed = jnp.zeros((2 * n_rows, 128), F32)
    for z in [op[1] for op in OPS if op[0] == "h"]:
        taken = zone - (block if z == 0 else 0)
        drain(back.at[pl.ds(0, taken), :], back_recv.at[z])
        span = pl.ds(z * zone, zone)
        summed = summed + jnp.dot(comb_w[:, span], back[span, :], preferred_element_type=F32)
    comb_out[...] = (summed[:n_rows] + summed[n_rows:]).astype(BF16)
    for step_y, other in tp_steps:
        to = at_tp(step_y, other)
        remote(
            comb_out.at[pl.ds(pl.multiple_of(to * own, own), own), :], comb_in.at[t],
            small_send.at[7], small_recv.at[4], tp=to,
        ).start()
    comb_in[t] = comb_out[pl.ds(pl.multiple_of(t * own, own), own), :]

    halo.wait_send()
    drain(w_in.at[0, pl.ds(0, n_tp - 1)], small_send.at[0])
    drain(w_in.at[pl.ds(0, dim_x - 1)], small_send.at[10])
    drain(s_in.at[pl.ds(0, n_tp - 1)], small_send.at[1])
    drain(mixed.at[pl.ds(0, 2 * dim_y - 1)], small_send.at[2])
    drain(squares.at[pl.ds(0, n_tp - 1)], small_send.at[3])
    drain(res_in.at[pl.ds(0, n_tp - 1)], small_send.at[4])
    drain(far_out, small_send.at[5])
    drain(near_out.at[:, pl.ds(0, len(NEAR) * zone - block), :], small_send.at[6])
    drain(near_out, small_send.at[8])
    drain(result.at[pl.ds(0, slots - block), :], small_send.at[9])
    for j, op in enumerate(OPS):
        if op[0] == "g":
            drain(norms.at[pl.ds(0, 7)], ring_send.at[j])
        else:
            drain(rows.at[0, pl.ds(0, 3), pl.ds(0, 5 * zone), :], ring_send.at[j])

    drain(res_in.at[pl.ds(0, n_tp - 1)], small_recv.at[3])
    drain(comb_in.at[pl.ds(0, n_tp - 1)], small_recv.at[4])
    drain(comb_in.at[pl.ds(0, n_tp - 1)], small_send.at[7])
    combined = jnp.concatenate([comb_in[k] for k in range(n_tp)], axis=1).astype(F32)
    kept = jnp.concatenate([res_in[k] for k in range(n_tp)], axis=1).astype(F32)
    mean = jnp.mean(combined * combined, axis=1, keepdims=True)
    out[...] = (kept + combined * lax.rsqrt(mean + EPS) * post_gain[...].astype(F32)[None, :]).astype(BF16)


def local(
    stream_in, pre_gate, value_in, post_gate, conv_taps, out_weight, route_ids, route_weight,
    ffn_gain, post_gain, gate_proj, up_proj, down_proj,
):
    n_sp, n_tp = lax.axis_size("sp"), lax.axis_size("tp")
    own, features = stream_in.shape
    n_rows = pre_gate.shape[0]
    cap = 2 * own * route_ids.shape[1] // n_sp
    slots = n_sp * n_tp * cap
    vmem = pl.BlockSpec(memory_space=pltpu.VMEM)
    hbm = pl.BlockSpec(memory_space=pl.ANY)
    dma = pltpu.SemaphoreType.DMA
    zone = 4 * n_tp * cap
    half_tp = n_tp // 2
    return pl.pallas_call(
        functools.partial(kernel, (n_sp, n_tp, 4, cap)),
        out_shape=jax.ShapeDtypeStruct(stream_in.shape, BF16),
        in_specs=[vmem] * 10 + [hbm] * 3,
        out_specs=vmem,
        scratch_shapes=[
            pltpu.VMEM((16, 128), BF16),
            pltpu.VMEM((16, 128), BF16),
            pltpu.VMEM((n_tp, n_rows // 2, 128), BF16),
            pltpu.VMEM((4, n_tp, 16, 128), BF16),
            pltpu.VMEM((n_tp * 128, 256), BF16),
            pltpu.VMEM((n_tp, own, 128), BF16),
            pltpu.VMEM((n_tp, 8, n_rows // 2), F32),
            pltpu.VMEM((slots, n_rows), BF16),
            pltpu.VMEM((2 * n_rows, slots), BF16),
            pltpu.VMEM((128, n_rows), F32),
            pltpu.VMEM((n_rows, 128), F32),
            pltpu.VMEM((half_tp, n_rows, 128), BF16),
            pltpu.VMEM((len(FAR) * zone, 128), BF16),
            pltpu.VMEM((half_tp, len(NEAR) * zone, 128), BF16),
            pltpu.VMEM((2, half_tp, slots, 128), BF16),
            pltpu.VMEM((2, half_tp, slots, 128), BF16),
            pltpu.VMEM((slots, 128), BF16),
            pltpu.VMEM((slots, 128), BF16),
            pltpu.VMEM((n_rows, 128), BF16),
            pltpu.VMEM((n_tp, own, 128), BF16),
            pltpu.VMEM((n_rows, 128), BF16),
            pltpu.VMEM((n_tp, own, 128), BF16),
            pltpu.VMEM((features, 256), BF16),
            pltpu.VMEM((features, 128), BF16),
            dma((3,)), dma((2,)), dma((11,)), dma((6,)), dma((8,)), dma((len(FAR),)),
            dma((len(NEAR),)), dma((len(NEAR),)),
            dma((len(OPS), 2, 4)), dma((len(OPS),)), dma((len(OPS),)), dma((8,)),
        ],
        compiler_params=pltpu.CompilerParams(
            collective_id=0, has_side_effects=True, vmem_limit_bytes=56 * 1024 * 1024
        ),
        cost_estimate=pl.CostEstimate(flops=4 * 10**9, bytes_accessed=3 * 10**6, transcendentals=0),
    )(
        stream_in, pre_gate.T, value_in.T, post_gate.T, conv_taps, out_weight,
        route_ids.T, route_weight.T,
        ffn_gain, post_gain,
        gate_proj, up_proj, down_proj,
    )


def solution(mesh):
    placed = (
        P(("sp", "tp"), None),
        P("sp", "tp"),
        P("sp", "tp"),
        P("sp", "tp"),
        P(None, "tp"),
        P("tp", None),
        P("sp", None),
        P("sp", None),
        P(),
        P(),
        P("sp", None, "tp"),
        P("sp", None, "tp"),
        P("sp", None, "tp"),
    )
    return jax.shard_map(
        local, mesh=mesh, in_specs=placed, out_specs=P(("sp", "tp"), None), check_vma=False
    )
```

```python
import functools

import jax
import jax.numpy as jnp
from jax import lax
from jax.experimental import pallas as pl
from jax.experimental.pallas import tpu as pltpu
from jax.sharding import PartitionSpec as P

MESH = pl.DeviceIdType.MESH
F32 = jnp.float32
BF16 = jnp.bfloat16
LIMIT = 7.0
SLOPE = 1.702
EPS = 1e-06
OFFSETS = (0, 1, -1, 2, -2, 3, -3, 4)
AT = {offset: place for place, offset in enumerate(OFFSETS)}
NEAR, FAR = (0, 1, 2, 3, 4), (5, 6, 7)
EARLY, LATE = (0, 1, 2), (3, 4)
FIRST_SLICES = 3
OPS = (('g', 0, 0), ('r', 5, 2), ('r', 6, 3), ('r', 7, 4), ('h', 5, 7), ('h', 6, 8), ('h', 7, 9), ('h', 0, 10), ('h', 1, 11), ('h', 2, 12), ('h', 3, 13), ('h', 4, 13))
WORK = {1: [('pick', 0)], 4: [('pick', 1)], 5: [('pick', 2)], 6: [('pick', 3), ('units', 5)], 7: [('units', 6)], 8: [('units', 7), ('across', 0)], 9: [('units', 0), ('across', 1)], 10: [('units', 1), ('across', 2)], 11: [('units', 2), ('across', 3), ('across', 4)], 12: [('units', 3), ('units', 4)], 13: [('weights', 0), ('weights', 1)], 14: [('weights', 2), ('weights', 3)]}


def kernel(
    cfg,
    stream_hbm, pre_hbm, value_hbm, post_hbm, taps_hbm, weight_hbm, ids_hbm, route_w_hbm,
    ffn_gain_hbm, post_gain_hbm, gate_hbm, up_hbm, down_hbm,
    out,
    stream, pre, value, post, taps, weight, ids, route_w, ffn_gain, post_gain, in_sem,
    halo_src, halo_dst, mixed, w_in, w_diag, s_in, squares, picker, comb_w, aux, slot_cols,
    norms, far_out, near_out, rows, hidden, result, back, res_keep, res_in, comb_out, comb_in, w_gu, w_down,
    load_sem, halo_sem, small_send, small_recv, mix_recv, far_recv, near_recv, near_pair,
    ring_recv, ring_pair, ring_send, back_recv,
):
    n_sp, n_tp, dim_x, cap = cfg
    dim_z, dim_y = n_sp // dim_x, n_tp // 2
    s, t = lax.axis_index("sp"), lax.axis_index("tp")
    sz, sx = s // dim_x, lax.rem(s, dim_x)
    y, core = t // 2, lax.rem(t, 2)
    n_rows = pre.shape[1]
    channels = pre.shape[0]
    top = ids.shape[0]
    own = n_rows // n_tp
    half = n_rows // 2
    block = own * cap * n_tp // own
    slots = block * n_sp
    zone = dim_x * block

    def at_tp(step_y, other_core):
        to_core = 1 - core if other_core else core
        return lax.rem(y + step_y + dim_y, dim_y) * 2 + to_core

    def remote(src, dst, send, recv, tp=None, sp=None):
        target = {"tp": tp} if sp is None else {"sp": sp}
        return pltpu.make_async_remote_copy(
            src_ref=src, dst_ref=dst, send_sem=send, recv_sem=recv,
            device_id=target, device_id_type=MESH,
        )

    def drain(ref, sem):
        pltpu.make_async_copy(ref, ref, sem).wait()

    def z_step(p):
        place = p // dim_x
        return (place + 1) // 2 if place % 2 else (dim_z - place // 2) % dim_z

    barrier = pltpu.get_barrier_semaphore()

    def greet_tp(step, carry):
        pl.semaphore_signal(
            barrier, inc=1, device_id={"tp": lax.rem(t + step, n_tp)}, device_id_type=MESH
        )
        return carry

    def greet_sp(step, carry):
        pl.semaphore_signal(
            barrier, inc=1, device_id={"sp": lax.rem(s + step, n_sp)}, device_id_type=MESH
        )
        return carry

    lax.fori_loop(n_sp // 4, n_sp - n_sp // 4, greet_sp, 0)
    lax.fori_loop(1, n_tp, greet_tp, 0)
    lax.fori_loop(1, n_sp // 4, greet_sp, 0)
    lax.fori_loop(n_sp - n_sp // 4, n_sp, greet_sp, 0)

    inputs = [
        pltpu.make_async_copy(there, here, in_sem.at[k])
        for k, (there, here) in enumerate((
            (pre_hbm, pre), (value_hbm, value), (post_hbm, post), (weight_hbm, weight),
            (taps_hbm, taps), (stream_hbm, stream), (ids_hbm, ids), (route_w_hbm, route_w),
            (ffn_gain_hbm, ffn_gain), (post_gain_hbm, post_gain),
        ))
    ]
    for copy in inputs:
        copy.start()
    for copy in inputs[:3]:
        copy.wait()

    gated = (pre[...].astype(F32) * value[...].astype(F32)).astype(BF16).astype(F32)
    gates = jnp.transpose(jnp.concatenate([gated, post[...].astype(F32)], axis=0))
    halo_src[...] = gates[n_rows - 16 :, :].astype(BF16)

    for copy in inputs[3:]:
        copy.wait()
    pl.semaphore_wait(barrier, n_tp + n_sp - 2)

    halo = remote(
        halo_src, halo_dst, halo_sem.at[0], halo_sem.at[1], sp=lax.rem(s + 1, n_sp)
    )
    halo.start()

    share = weight.shape[0] // dim_x
    quarter = pl.ds(pl.multiple_of(sx * share, share), share)
    tp_steps = [(d, o) for d in (4, 3, 5, 2, 6, 1, 7) for o in (False, True)] + [(0, True)]
    for step_y, other in tp_steps:
        to = at_tp(step_y, other)
        piece = pl.ds(pl.multiple_of(to * 128, 128), 128)
        remote(
            weight.at[quarter, piece], w_in.at[sx, t], small_send.at[0], small_recv.at[0], tp=to
        ).start()
    own_cols = pl.ds(pl.multiple_of(t * 128, 128), 128)
    w_in[sx, t] = weight[quarter, own_cols]
    s_in[t] = stream[:, own_cols]

    wide, second = gates[:, :channels], gates[:, channels:]
    tap = taps[...].astype(F32)
    shift_1, shift_2 = pltpu.roll(wide, 1, 0), pltpu.roll(wide, 2, 0)

    def mixer_rows(two_back, one_back, here, gate):
        convolved = tap[0:1] * two_back
        convolved = convolved + tap[1:2] * one_back
        convolved = convolved + tap[2:3] * here
        return gate * convolved

    mixer = mixer_rows(shift_2, shift_1, wide, second)
    body = pl.ds(16, half - 16)
    head = pl.ds(0, 16)
    mixed[t, body, :] = jnp.concatenate([mixer[16:half], mixer[half + 16 :]], axis=1).astype(BF16)

    steps = (4, 3, 5, 2, 6, 1, 7)
    own_body = mixed.at[t, body, :]
    for step_y in steps:
        remote(
            own_body, own_body, small_send.at[2], mix_recv.at[step_y], tp=at_tp(step_y, False)
        ).start()
    partner = at_tp(0, True)
    remote(own_body, own_body, small_send.at[2], mix_recv.at[0], tp=partner).start()
    for step_y, other in tp_steps:
        to = at_tp(step_y, other)
        piece = pl.ds(pl.multiple_of(to * 128, 128), 128)
        remote(stream.at[:, piece], s_in.at[t], small_send.at[1], small_recv.at[1], tp=to).start()
    aux[...] = jnp.zeros_like(aux)
    aux[0:top, :] = ids[...].astype(F32)
    aux[top : 2 * top, :] = route_w[...]
    by_row = jnp.transpose(aux[...])
    id_cols = [by_row[:, k : k + 1] for k in range(top)]
    amounts = [by_row[:, top + k : top + k + 1] for k in range(top)]
    lane = lax.broadcasted_iota(jnp.int32, (n_rows, 128), 1)
    lane_f = lane.astype(F32)
    named = jnp.zeros((n_rows, 128), F32)
    for k in range(top):
        named = named + jnp.where(id_cols[k] == lane_f, 1.0, 0.0)
    row_a = lax.broadcasted_iota(jnp.int32, (n_rows, n_rows), 0)
    row_b = lax.broadcasted_iota(jnp.int32, (n_rows, n_rows), 1)
    earlier = jnp.where((row_a > row_b) & (row_a // own == row_b // own), 1.0, 0.0).astype(BF16)
    rank = jnp.dot(earlier, named.astype(BF16), preferred_element_type=F32)
    dz = lax.rem(sz - lane // dim_x + 32 * dim_z, dim_z)
    dx = lax.rem(sx - lax.rem(lane, dim_x) + 32 * dim_x, dim_x)
    z_place = jnp.where(dz * 2 <= dim_z, jnp.maximum(2 * dz - 1, 0), 2 * (dim_z - dz))
    at_row = lax.broadcasted_iota(jnp.int32, (n_rows, 128), 0)
    slot_of = ((z_place * dim_x + dx) * block + (at_row // own) * cap).astype(F32) + rank
    places = [
        jnp.sum(jnp.where(id_cols[k] == lane_f, slot_of, 0.0), axis=1, keepdims=True)
        for k in range(top)
    ]
    columns = jnp.zeros((n_rows, 128), F32)
    for k in range(top):
        columns = jnp.where(lane == k, places[k], columns)
        columns = jnp.where(lane == top + k, amounts[k], columns)
    slot_cols[...] = columns
    slot_rows = jnp.transpose(columns)
    w_diag[...] = jnp.zeros_like(w_diag)

    row_no = lax.broadcasted_iota(jnp.int32, (16, channels), 0)
    halo.wait_recv()
    rim = halo_dst[...].astype(F32)[:, :channels]
    rim = jnp.where(s > 0, rim, 0.0)
    last, before_last = rim[15:16, :], rim[14:15, :]
    one_back = jnp.where(row_no == 0, last, shift_1[:16])
    two_back = jnp.where(row_no == 0, before_last, jnp.where(row_no == 1, last, shift_2[:16]))
    first_rows = mixer_rows(two_back, one_back, wide[:16], second[:16])
    mixed[t, head, :] = jnp.concatenate([first_rows, mixer[half : half + 16]], axis=1).astype(BF16)
    own_head = mixed.at[t, head, :]
    for step_y, other in tp_steps:
        remote(
            own_head, own_head, small_send.at[11], small_recv.at[6], tp=at_tp(step_y, other)
        ).start()
    for core_no in range(2):
        for place, offset in enumerate(OFFSETS):
            origin = pl.ds(pl.multiple_of(at_tp(offset, core_no == 1) * 128, 128), 128)
            here = pl.ds((core_no * dim_y + place) * 128, 128)
            pltpu.make_async_copy(
                gate_hbm.at[0, origin, :], w_gu.at[here, pl.ds(0, 128)], load_sem.at[0]
            ).start()
            pltpu.make_async_copy(
                up_hbm.at[0, origin, :], w_gu.at[here, pl.ds(128, 128)], load_sem.at[1]
            ).start()
            pltpu.make_async_copy(
                down_hbm.at[0, origin, :], w_down.at[here, :], load_sem.at[2]
            ).start()

    drain(w_in.at[sx, pl.ds(0, n_tp - 1)], small_recv.at[0])
    for step_x in (2, 1, 3):
        remote(
            w_in.at[sx], w_in.at[sx], small_send.at[10], small_recv.at[5],
            sp=sz * dim_x + lax.rem(sx + step_x, dim_x),
        ).start()

    def fill_picker(part, carry):
        first = pl.multiple_of(part * 256, 256)
        number = lax.broadcasted_iota(jnp.int32, (256, n_rows), 0) + part * 256
        number = number.astype(F32)
        hit = number == slot_rows[0:1, :]
        for k in range(1, top):
            hit = hit | (number == slot_rows[k : k + 1, :])
        picker[pl.ds(first, 256), :] = jnp.where(hit, 1.0, 0.0).astype(BF16)
        return carry

    lax.fori_loop(0, slots // 256, fill_picker, 0)

    drain(w_in.at[pl.ds(0, dim_x - 1)], small_recv.at[5])
    for k in range(n_tp):
        piece = jnp.concatenate([w_in[x, k] for x in range(dim_x)], axis=0)
        w_diag[pl.ds(k * 128, 64), pl.ds(0, 128)] = piece
        w_diag[pl.ds(k * 128 + 64, 64), pl.ds(128, 128)] = piece
    for step_y in steps:
        arrived = mixed.at[at_tp(-step_y, False), body, :]
        drain(arrived, mix_recv.at[step_y])
        remote(arrived, arrived, small_send.at[2], mix_recv.at[0], tp=partner).start()
    drain(s_in.at[pl.ds(0, n_tp - 1)], small_recv.at[1])
    drain(mixed.at[pl.ds(0, dim_y), body, :], mix_recv.at[0])
    drain(mixed.at[pl.ds(0, n_tp - 1), head, :], small_recv.at[6])
    stacked = jnp.concatenate([mixed[k] for k in range(n_tp)], axis=1)
    projected = jnp.dot(stacked, w_diag[...], preferred_element_type=F32)
    projected = jnp.concatenate([projected[:, :128], projected[:, 128:]], axis=0)
    residual = (s_in[...].reshape(n_rows, 128).astype(F32) + projected).astype(BF16)
    res_keep[...] = residual
    res = residual.astype(F32)

    sums = jnp.sum(res * res, axis=1, keepdims=True)
    across = jnp.transpose(jnp.broadcast_to(sums, (n_rows, 128)))
    first_row = lax.broadcasted_iota(jnp.int32, (8, half), 0) == 0
    squares[t] = jnp.where(first_row, across[0:8, :half], across[0:8, half:])
    for step_y, other in tp_steps:
        remote(
            squares.at[t], squares.at[t], small_send.at[3], small_recv.at[2],
            tp=at_tp(step_y, other),
        ).start()
    drain(squares.at[pl.ds(0, n_tp - 1)], small_recv.at[2])
    total = squares[0]
    for k in range(1, n_tp):
        total = total + squares[k]
    scale = lax.rsqrt(total / (n_tp * 128) + EPS)
    scale = jnp.concatenate(
        [jnp.transpose(jnp.broadcast_to(scale[k : k + 1, :], (half, half))) for k in range(2)], axis=0
    )
    gains = ffn_gain[...].astype(F32).reshape(n_tp, 128)
    gain_no = lax.broadcasted_iota(jnp.int32, (n_tp, 128), 0)
    gain = jnp.sum(jnp.where(gain_no == t, gains, 0.0), axis=0, keepdims=True)
    normed = (res * scale * gain).astype(BF16)

    norms[0] = normed

    right, left = at_tp(1, False), at_tp(-1, False)
    lower, upper = zone // 2, zone - zone // 2

    def ring_step(j, d):
        kind, z, _ = OPS[j]
        base = 0 if kind == "g" else z * zone

        def part(place, span, core_no=0):
            first, size = span
            span = pl.ds(base + first, size)
            if kind == "g":
                return norms.at[place, span, :]
            return (rows if kind == "r" else hidden).at[core_no, place, span, :]

        def pass_on(origin, shifted, span, to, sem):
            remote(part(origin, span), part(shifted, span), ring_send.at[j], sem, tp=to).start()

        def cross(place, span):
            if kind != "g":
                remote(
                    part(place, span), part(place, span, 1), ring_send.at[j], ring_pair.at[j],
                    tp=partner,
                ).start()

        full, first, second = (0, zone), (0, lower), (lower, upper)
        if d == 0:
            if kind == "r":
                drain(part(0, full), far_recv.at[z - FAR[0]])
            pass_on(AT[0], AT[-1], full, right, ring_recv.at[j, 0, 0])
            pass_on(AT[0], AT[1], full, left, ring_recv.at[j, 1, 0])
            cross(AT[0], full)
            return
        for way, sign, ahead, end in ((0, -1, right, first), (1, 1, left, second)):
            origin = AT[sign * d] if d < 4 else AT[4]
            span = full if d < 4 else end
            drain(part(origin, span), ring_recv.at[j, way, d - 1])
            if d < 4:
                shifted = AT[sign * (d + 1)] if d < 3 else AT[4]
                pass_on(origin, shifted, full if d < 3 else end, ahead, ring_recv.at[j, way, d])
            cross(origin, span)
        if d == 4 and kind != "g":
            drain(
                (rows if kind == "r" else hidden).at[1, :, pl.ds(base, zone), :], ring_pair.at[j]
            )

    ring_step(0, 0)

    def expert_of(p):
        to_z = lax.rem(sz - z_step(p) + dim_z, dim_z)
        return to_z * dim_x + lax.rem(sx - p % dim_x + dim_x, dim_x)

    for z in FAR:
        base = (z - FAR[0]) * zone
        far_out[pl.ds(base, zone), :] = jnp.dot(
            picker[pl.ds(z * zone, zone), :], normed, preferred_element_type=F32
        ).astype(BF16)
        for x in range(dim_x):
            p = z * dim_x + x
            remote(
                far_out.at[pl.ds(base + x * block, block), :],
                rows.at[0, 0, pl.ds(p * block, block), :],
                small_send.at[5], far_recv.at[z - FAR[0]], sp=expert_of(p),
            ).start()

    def pick_zone(z, first, last):
        span = pl.ds(z * zone, zone)
        wide_rows = jnp.concatenate([norms[k] for k in range(first, last)], axis=1)
        picked = jnp.dot(picker[span, :], wide_rows, preferred_element_type=F32).astype(BF16)
        for k in range(first, last):
            piece = picked[:, (k - first) * 128 : (k - first + 1) * 128]
            near_out[k, span, :] = piece
            if z == 0:
                rows[0, k, pl.ds(0, block), :] = piece[:block]
        for x in range(dim_x):
            p = z * dim_x + x
            if p == 0:
                continue
            place = pl.ds(p * block, block)
            remote(
                near_out.at[pl.ds(first, last - first), place, :],
                rows.at[0, pl.ds(first, last - first), place, :],
                small_send.at[6], near_recv.at[z], sp=expert_of(p),
            ).start()

    def pick(batch):
        if batch == 0:
            for z in EARLY:
                pick_zone(z, 0, FIRST_SLICES)
            return
        if batch == 1:
            for z in EARLY:
                pick_zone(z, FIRST_SLICES, dim_y)
            return
        pick_zone(LATE[batch - 2], 0, dim_y)

    def across(z):
        own_x = 1 if z == 0 else 0
        taken = pl.ds(z * zone, zone - own_x * block)
        drain(rows.at[0, :, taken, :], near_recv.at[z])
        span = pl.ds(z * zone, zone)
        remote(
            rows.at[0, :, span, :], rows.at[1, :, span, :], small_send.at[8], near_pair.at[z],
            tp=partner,
        ).start()

    for step_y, other in tp_steps:
        to = at_tp(step_y, other)
        remote(
            res_keep.at[pl.ds(pl.multiple_of(to * own, own), own), :], res_in.at[t],
            small_send.at[4], small_recv.at[3], tp=to,
        ).start()
    res_in[t] = res_keep[pl.ds(pl.multiple_of(t * own, own), own), :]

    def fill_weights(part, carry):
        first = pl.multiple_of(part * 256, 256)
        number = lax.broadcasted_iota(jnp.int32, (n_rows, 256), 1) + part * 256
        number = number.astype(F32)
        columns = slot_cols[...]
        summed = jnp.zeros((n_rows, 256), F32)
        for k in range(top):
            summed = summed + jnp.where(
                number == columns[:, k : k + 1], columns[:, top + k : top + k + 1], 0.0
            )
        high = summed.astype(BF16)
        comb_w[pl.ds(0, n_rows), pl.ds(first, 256)] = high
        comb_w[pl.ds(n_rows, n_rows), pl.ds(first, 256)] = (summed - high.astype(F32)).astype(BF16)
        return carry

    def weights(z):
        lax.fori_loop(z * (slots // 1024), (z + 1) * (slots // 1024), fill_weights, 0)

    drain(w_gu.at[:, pl.ds(0, 128)], load_sem.at[0])
    drain(w_gu.at[:, pl.ds(128, 128)], load_sem.at[1])
    drain(w_down, load_sem.at[2])

    def stacked_rows(held, z):
        span = pl.ds(z * zone, zone)
        return jnp.concatenate(
            [held[core_no, k, span, :] for core_no in range(2) for k in range(dim_y)], axis=1
        )

    def units(z):
        span = pl.ds(z * zone, zone)
        if z in NEAR:
            drain(rows.at[1, :, span, :], near_pair.at[z])
        both = jnp.dot(stacked_rows(rows, z), w_gu[...], preferred_element_type=F32)
        gate = jnp.minimum(both[:, :128], LIMIT)
        up = jnp.clip(both[:, 128:], -LIMIT, LIMIT)
        hidden[0, 0, span, :] = ((up + 1.0) * (gate * jax.nn.sigmoid(SLOPE * gate))).astype(BF16)

    def outputs(z):
        span = pl.ds(z * zone, zone)
        done = jnp.dot(stacked_rows(hidden, z), w_down[...], preferred_element_type=F32)
        result[span, :] = done.astype(BF16)
        for x in range(dim_x):
            p = z * dim_x + x
            place = pl.ds(p * block, block)
            if p == 0:
                back[place, :] = result[place, :]
                continue
            to_z = lax.rem(sz + z_step(p), dim_z)
            to_x = lax.rem(sx + x, dim_x)
            remote(
                result.at[place, :], back.at[place, :], small_send.at[9], back_recv.at[z],
                sp=to_z * dim_x + to_x,
            ).start()

    tasks = dict(pick=pick, weights=weights, across=across, units=units)
    for slot in range(max(op[2] for op in OPS) + 5):
        finished = []
        for j, (kind, z, start) in reversed(list(enumerate(OPS))):
            d = slot - start
            if 0 <= d <= 4 and (j, d) != (0, 0):
                ring_step(j, d)
                if d == 4 and kind == "h":
                    finished.append(z)
        for name, z in WORK.get(slot, ()):
            tasks[name](z)
        for z in finished:
            outputs(z)

    summed = jnp.zeros((2 * n_rows, 128), F32)
    for z in [op[1] for op in OPS if op[0] == "h"]:
        taken = zone - (block if z == 0 else 0)
        drain(back.at[pl.ds(0, taken), :], back_recv.at[z])
        span = pl.ds(z * zone, zone)
        summed = summed + jnp.dot(comb_w[:, span], back[span, :], preferred_element_type=F32)
    comb_out[...] = (summed[:n_rows] + summed[n_rows:]).astype(BF16)
    for step_y, other in tp_steps:
        to = at_tp(step_y, other)
        remote(
            comb_out.at[pl.ds(pl.multiple_of(to * own, own), own), :], comb_in.at[t],
            small_send.at[7], small_recv.at[4], tp=to,
        ).start()
    comb_in[t] = comb_out[pl.ds(pl.multiple_of(t * own, own), own), :]

    halo.wait_send()
    drain(w_in.at[0, pl.ds(0, n_tp - 1)], small_send.at[0])
    drain(w_in.at[pl.ds(0, dim_x - 1)], small_send.at[10])
    drain(s_in.at[pl.ds(0, n_tp - 1)], small_send.at[1])
    drain(mixed.at[pl.ds(0, 2 * dim_y - 1), body, :], small_send.at[2])
    drain(mixed.at[pl.ds(0, n_tp - 1), head, :], small_send.at[11])
    drain(squares.at[pl.ds(0, n_tp - 1)], small_send.at[3])
    drain(res_in.at[pl.ds(0, n_tp - 1)], small_send.at[4])
    drain(far_out, small_send.at[5])
    drain(near_out.at[:, pl.ds(0, len(NEAR) * zone - block), :], small_send.at[6])
    drain(near_out, small_send.at[8])
    drain(result.at[pl.ds(0, slots - block), :], small_send.at[9])
    for j, op in enumerate(OPS):
        if op[0] == "g":
            drain(norms.at[pl.ds(0, 7)], ring_send.at[j])
        else:
            drain(rows.at[0, pl.ds(0, 3), pl.ds(0, 5 * zone), :], ring_send.at[j])

    drain(res_in.at[pl.ds(0, n_tp - 1)], small_recv.at[3])
    drain(comb_in.at[pl.ds(0, n_tp - 1)], small_recv.at[4])
    drain(comb_in.at[pl.ds(0, n_tp - 1)], small_send.at[7])
    combined = jnp.concatenate([comb_in[k] for k in range(n_tp)], axis=1).astype(F32)
    kept = jnp.concatenate([res_in[k] for k in range(n_tp)], axis=1).astype(F32)
    mean = jnp.mean(combined * combined, axis=1, keepdims=True)
    out[...] = (kept + combined * lax.rsqrt(mean + EPS) * post_gain[...].astype(F32)[None, :]).astype(BF16)


def local(
    stream_in, pre_gate, value_in, post_gate, conv_taps, out_weight, route_ids, route_weight,
    ffn_gain, post_gain, gate_proj, up_proj, down_proj,
):
    n_sp, n_tp = lax.axis_size("sp"), lax.axis_size("tp")
    own, features = stream_in.shape
    n_rows = pre_gate.shape[0]
    cap = 2 * own * route_ids.shape[1] // n_sp
    slots = n_sp * n_tp * cap
    vmem = pl.BlockSpec(memory_space=pltpu.VMEM)
    hbm = pl.BlockSpec(memory_space=pl.ANY)
    dma = pltpu.SemaphoreType.DMA
    zone = 4 * n_tp * cap
    half_tp = n_tp // 2
    return pl.pallas_call(
        functools.partial(kernel, (n_sp, n_tp, 4, cap)),
        out_shape=jax.ShapeDtypeStruct(stream_in.shape, BF16),
        in_specs=[hbm] * 13,
        out_specs=vmem,
        scratch_shapes=[
            pltpu.VMEM(stream_in.shape, BF16),
            pltpu.VMEM(pre_gate.shape[::-1], BF16),
            pltpu.VMEM(pre_gate.shape[::-1], BF16),
            pltpu.VMEM(pre_gate.shape[::-1], BF16),
            pltpu.VMEM(conv_taps.shape, BF16),
            pltpu.VMEM(out_weight.shape, BF16),
            pltpu.VMEM(route_ids.shape[::-1], jnp.int32),
            pltpu.VMEM(route_weight.shape[::-1], F32),
            pltpu.VMEM(ffn_gain.shape, BF16),
            pltpu.VMEM(post_gain.shape, BF16),
            dma((10,)),
            pltpu.VMEM((16, 128), BF16),
            pltpu.VMEM((16, 128), BF16),
            pltpu.VMEM((n_tp, n_rows // 2, 128), BF16),
            pltpu.VMEM((4, n_tp, 16, 128), BF16),
            pltpu.VMEM((n_tp * 128, 256), BF16),
            pltpu.VMEM((n_tp, own, 128), BF16),
            pltpu.VMEM((n_tp, 8, n_rows // 2), F32),
            pltpu.VMEM((slots, n_rows), BF16),
            pltpu.VMEM((2 * n_rows, slots), BF16),
            pltpu.VMEM((128, n_rows), F32),
            pltpu.VMEM((n_rows, 128), F32),
            pltpu.VMEM((half_tp, n_rows, 128), BF16),
            pltpu.VMEM((len(FAR) * zone, 128), BF16),
            pltpu.VMEM((half_tp, len(NEAR) * zone, 128), BF16),
            pltpu.VMEM((2, half_tp, slots, 128), BF16),
            pltpu.VMEM((2, half_tp, slots, 128), BF16),
            pltpu.VMEM((slots, 128), BF16),
            pltpu.VMEM((slots, 128), BF16),
            pltpu.VMEM((n_rows, 128), BF16),
            pltpu.VMEM((n_tp, own, 128), BF16),
            pltpu.VMEM((n_rows, 128), BF16),
            pltpu.VMEM((n_tp, own, 128), BF16),
            pltpu.VMEM((features, 256), BF16),
            pltpu.VMEM((features, 128), BF16),
            dma((3,)), dma((2,)), dma((12,)), dma((7,)), dma((8,)), dma((len(FAR),)),
            dma((len(NEAR),)), dma((len(NEAR),)),
            dma((len(OPS), 2, 4)), dma((len(OPS),)), dma((len(OPS),)), dma((8,)),
        ],
        compiler_params=pltpu.CompilerParams(
            collective_id=0, has_side_effects=True, vmem_limit_bytes=63 * 1024 * 1024
        ),
        cost_estimate=pl.CostEstimate(flops=4 * 10**9, bytes_accessed=3 * 10**6, transcendentals=0),
    )(
        stream_in, pre_gate.T, value_in.T, post_gate.T, conv_taps, out_weight,
        route_ids.T, route_weight.T,
        ffn_gain, post_gain,
        gate_proj, up_proj, down_proj,
    )


def solution(mesh):
    placed = (
        P(("sp", "tp"), None),
        P("sp", "tp"),
        P("sp", "tp"),
        P("sp", "tp"),
        P(None, "tp"),
        P("tp", None),
        P("sp", None),
        P("sp", None),
        P(),
        P(),
        P("sp", None, "tp"),
        P("sp", None, "tp"),
        P("sp", None, "tp"),
    )
    return jax.shard_map(
        local, mesh=mesh, in_specs=placed, out_specs=P(("sp", "tp"), None), check_vma=False
    )
```

```python
import functools

import jax
import jax.numpy as jnp
from jax import lax
from jax.experimental import pallas as pl
from jax.experimental.pallas import tpu as pltpu
from jax.sharding import PartitionSpec as P

MESH = pl.DeviceIdType.MESH
F32 = jnp.float32
BF16 = jnp.bfloat16
LIMIT = 7.0
SLOPE = 1.702
EPS = 1e-06
OFFSETS = (0, 1, -1, 2, -2, 3, -3, 4)
AT = {offset: place for place, offset in enumerate(OFFSETS)}
NEAR, FAR = (0, 1, 2, 3, 4), (5, 6, 7)
EARLY, LATE = (0, 1, 2), (3, 4)
FIRST_SLICES = 3
OPS = (('g', 0, 0), ('r', 5, 2), ('r', 6, 3), ('r', 7, 6), ('h', 5, 7), ('h', 6, 8), ('h', 0, 9), ('h', 1, 10), ('h', 7, 11), ('h', 2, 12), ('h', 3, 13), ('h', 4, 13))
WORK = {1: [('pick', 0)], 4: [('pick', 1)], 5: [('pick', 2)], 6: [('pick', 3), ('units', 5)], 13: [('weights', 0), ('weights', 1)], 14: [('weights', 2), ('weights', 3)], 7: [('units', 6), ('across', 0)], 8: [('units', 0), ('across', 1)], 9: [('units', 1)], 10: [('units', 7), ('across', 2)], 11: [('units', 2), ('across', 3), ('across', 4)], 12: [('units', 3), ('units', 4)]}


def kernel(
    cfg,
    stream_hbm, pre_hbm, value_hbm, post_hbm, taps_hbm, weight_hbm, ids_hbm, route_w_hbm,
    ffn_gain_hbm, post_gain_hbm, gate_hbm, up_hbm, down_hbm,
    out,
    stream, pre, value, post, taps, weight, ids, route_w, ffn_gain, post_gain, in_sem,
    halo_src, halo_dst, mixed, w_in, w_diag, s_in, squares, picker, comb_w, aux, slot_cols,
    norms, far_out, near_out, rows, hidden, result, back, res_keep, res_in, comb_out, comb_in, w_gu, w_down,
    load_sem, halo_sem, small_send, small_recv, mix_recv, far_recv, near_recv, near_pair,
    ring_recv, ring_pair, ring_send, back_recv,
):
    n_sp, n_tp, dim_x, cap = cfg
    dim_z, dim_y = n_sp // dim_x, n_tp // 2
    s, t = lax.axis_index("sp"), lax.axis_index("tp")
    sz, sx = s // dim_x, lax.rem(s, dim_x)
    y, core = t // 2, lax.rem(t, 2)
    n_rows = pre.shape[1]
    channels = pre.shape[0]
    top = ids.shape[0]
    own = n_rows // n_tp
    half = n_rows // 2
    block = own * cap * n_tp // own
    slots = block * n_sp
    zone = dim_x * block

    def at_tp(step_y, other_core):
        to_core = 1 - core if other_core else core
        return lax.rem(y + step_y + dim_y, dim_y) * 2 + to_core

    def remote(src, dst, send, recv, tp=None, sp=None):
        target = {"tp": tp} if sp is None else {"sp": sp}
        return pltpu.make_async_remote_copy(
            src_ref=src, dst_ref=dst, send_sem=send, recv_sem=recv,
            device_id=target, device_id_type=MESH,
        )

    def drain(ref, sem):
        pltpu.make_async_copy(ref, ref, sem).wait()

    def z_step(p):
        place = p // dim_x
        return (place + 1) // 2 if place % 2 else (dim_z - place // 2) % dim_z

    barrier = pltpu.get_barrier_semaphore()

    def greet_tp(step, carry):
        pl.semaphore_signal(
            barrier, inc=1, device_id={"tp": lax.rem(t + step, n_tp)}, device_id_type=MESH
        )
        return carry

    def greet_sp(step, carry):
        pl.semaphore_signal(
            barrier, inc=1, device_id={"sp": lax.rem(s + step, n_sp)}, device_id_type=MESH
        )
        return carry

    lax.fori_loop(n_sp // 4, n_sp - n_sp // 4, greet_sp, 0)
    lax.fori_loop(1, n_tp, greet_tp, 0)
    lax.fori_loop(1, n_sp // 4, greet_sp, 0)
    lax.fori_loop(n_sp - n_sp // 4, n_sp, greet_sp, 0)

    inputs = [
        pltpu.make_async_copy(there, here, in_sem.at[k])
        for k, (there, here) in enumerate((
            (pre_hbm, pre), (value_hbm, value), (post_hbm, post), (weight_hbm, weight),
            (taps_hbm, taps), (stream_hbm, stream), (ids_hbm, ids), (route_w_hbm, route_w),
            (ffn_gain_hbm, ffn_gain), (post_gain_hbm, post_gain),
        ))
    ]
    for copy in inputs:
        copy.start()
    for copy in inputs[:3]:
        copy.wait()

    gated = (pre[...].astype(F32) * value[...].astype(F32)).astype(BF16).astype(F32)
    gates = jnp.transpose(jnp.concatenate([gated, post[...].astype(F32)], axis=0))
    halo_src[...] = gates[n_rows - 16 :, :].astype(BF16)

    for copy in inputs[3:]:
        copy.wait()
    pl.semaphore_wait(barrier, n_tp + n_sp - 2)

    halo = remote(
        halo_src, halo_dst, halo_sem.at[0], halo_sem.at[1], sp=lax.rem(s + 1, n_sp)
    )
    halo.start()

    share = weight.shape[0] // dim_x
    quarter = pl.ds(pl.multiple_of(sx * share, share), share)
    tp_steps = [(d, o) for d in (4, 3, 5, 2, 6, 1, 7) for o in (False, True)] + [(0, True)]
    for step_y, other in tp_steps:
        to = at_tp(step_y, other)
        piece = pl.ds(pl.multiple_of(to * 128, 128), 128)
        remote(
            weight.at[quarter, piece], w_in.at[sx, t], small_send.at[0], small_recv.at[0], tp=to
        ).start()
    own_cols = pl.ds(pl.multiple_of(t * 128, 128), 128)
    w_in[sx, t] = weight[quarter, own_cols]
    s_in[t] = stream[:, own_cols]

    wide, second = gates[:, :channels], gates[:, channels:]
    tap = taps[...].astype(F32)
    shift_1, shift_2 = pltpu.roll(wide, 1, 0), pltpu.roll(wide, 2, 0)

    def mixer_rows(two_back, one_back, here, gate):
        convolved = tap[0:1] * two_back
        convolved = convolved + tap[1:2] * one_back
        convolved = convolved + tap[2:3] * here
        return gate * convolved

    mixer = mixer_rows(shift_2, shift_1, wide, second)
    body = pl.ds(16, half - 16)
    head = pl.ds(0, 16)
    mixed[t, body, :] = jnp.concatenate([mixer[16:half], mixer[half + 16 :]], axis=1).astype(BF16)

    steps = (4, 3, 5, 2, 6, 1, 7)
    own_body = mixed.at[t, body, :]
    for step_y in steps:
        remote(
            own_body, own_body, small_send.at[2], mix_recv.at[step_y], tp=at_tp(step_y, False)
        ).start()
    partner = at_tp(0, True)
    remote(own_body, own_body, small_send.at[2], mix_recv.at[0], tp=partner).start()
    for step_y, other in tp_steps:
        to = at_tp(step_y, other)
        piece = pl.ds(pl.multiple_of(to * 128, 128), 128)
        remote(stream.at[:, piece], s_in.at[t], small_send.at[1], small_recv.at[1], tp=to).start()
    aux[...] = jnp.zeros_like(aux)
    aux[0:top, :] = ids[...].astype(F32)
    aux[top : 2 * top, :] = route_w[...]
    by_row = jnp.transpose(aux[...])
    id_cols = [by_row[:, k : k + 1] for k in range(top)]
    amounts = [by_row[:, top + k : top + k + 1] for k in range(top)]
    lane = lax.broadcasted_iota(jnp.int32, (n_rows, 128), 1)
    lane_f = lane.astype(F32)
    named = jnp.zeros((n_rows, 128), F32)
    for k in range(top):
        named = named + jnp.where(id_cols[k] == lane_f, 1.0, 0.0)
    row_a = lax.broadcasted_iota(jnp.int32, (n_rows, n_rows), 0)
    row_b = lax.broadcasted_iota(jnp.int32, (n_rows, n_rows), 1)
    earlier = jnp.where((row_a > row_b) & (row_a // own == row_b // own), 1.0, 0.0).astype(BF16)
    rank = jnp.dot(earlier, named.astype(BF16), preferred_element_type=F32)
    dz = lax.rem(sz - lane // dim_x + 32 * dim_z, dim_z)
    dx = lax.rem(sx - lax.rem(lane, dim_x) + 32 * dim_x, dim_x)
    z_place = jnp.where(dz * 2 <= dim_z, jnp.maximum(2 * dz - 1, 0), 2 * (dim_z - dz))
    at_row = lax.broadcasted_iota(jnp.int32, (n_rows, 128), 0)
    slot_of = ((z_place * dim_x + dx) * block + (at_row // own) * cap).astype(F32) + rank
    places = [
        jnp.sum(jnp.where(id_cols[k] == lane_f, slot_of, 0.0), axis=1, keepdims=True)
        for k in range(top)
    ]
    columns = jnp.zeros((n_rows, 128), F32)
    for k in range(top):
        columns = jnp.where(lane == k, places[k], columns)
        columns = jnp.where(lane == top + k, amounts[k], columns)
    slot_cols[...] = columns
    slot_rows = jnp.transpose(columns)
    w_diag[...] = jnp.zeros_like(w_diag)

    row_no = lax.broadcasted_iota(jnp.int32, (16, channels), 0)
    halo.wait_recv()
    rim = halo_dst[...].astype(F32)[:, :channels]
    rim = jnp.where(s > 0, rim, 0.0)
    last, before_last = rim[15:16, :], rim[14:15, :]
    one_back = jnp.where(row_no == 0, last, shift_1[:16])
    two_back = jnp.where(row_no == 0, before_last, jnp.where(row_no == 1, last, shift_2[:16]))
    first_rows = mixer_rows(two_back, one_back, wide[:16], second[:16])
    mixed[t, head, :] = jnp.concatenate([first_rows, mixer[half : half + 16]], axis=1).astype(BF16)
    own_head = mixed.at[t, head, :]
    for step_y, other in tp_steps:
        remote(
            own_head, own_head, small_send.at[11], small_recv.at[6], tp=at_tp(step_y, other)
        ).start()
    for core_no in range(2):
        for place, offset in enumerate(OFFSETS):
            origin = pl.ds(pl.multiple_of(at_tp(offset, core_no == 1) * 128, 128), 128)
            here = pl.ds((core_no * dim_y + place) * 128, 128)
            pltpu.make_async_copy(
                gate_hbm.at[0, origin, :], w_gu.at[here, pl.ds(0, 128)], load_sem.at[0]
            ).start()
            pltpu.make_async_copy(
                up_hbm.at[0, origin, :], w_gu.at[here, pl.ds(128, 128)], load_sem.at[1]
            ).start()
            pltpu.make_async_copy(
                down_hbm.at[0, origin, :], w_down.at[here, :], load_sem.at[2]
            ).start()

    drain(w_in.at[sx, pl.ds(0, n_tp - 1)], small_recv.at[0])
    for step_x in (2, 1, 3):
        remote(
            w_in.at[sx], w_in.at[sx], small_send.at[10], small_recv.at[5],
            sp=sz * dim_x + lax.rem(sx + step_x, dim_x),
        ).start()

    def fill_picker(part, carry):
        first = pl.multiple_of(part * 256, 256)
        number = lax.broadcasted_iota(jnp.int32, (256, n_rows), 0) + part * 256
        number = number.astype(F32)
        hit = number == slot_rows[0:1, :]
        for k in range(1, top):
            hit = hit | (number == slot_rows[k : k + 1, :])
        picker[pl.ds(first, 256), :] = jnp.where(hit, 1.0, 0.0).astype(BF16)
        return carry

    lax.fori_loop(0, slots // 256, fill_picker, 0)

    drain(w_in.at[pl.ds(0, dim_x - 1)], small_recv.at[5])
    for k in range(n_tp):
        piece = jnp.concatenate([w_in[x, k] for x in range(dim_x)], axis=0)
        w_diag[pl.ds(k * 128, 64), pl.ds(0, 128)] = piece
        w_diag[pl.ds(k * 128 + 64, 64), pl.ds(128, 128)] = piece
    for step_y in steps:
        arrived = mixed.at[at_tp(-step_y, False), body, :]
        drain(arrived, mix_recv.at[step_y])
        remote(arrived, arrived, small_send.at[2], mix_recv.at[0], tp=partner).start()
    drain(s_in.at[pl.ds(0, n_tp - 1)], small_recv.at[1])
    drain(mixed.at[pl.ds(0, dim_y), body, :], mix_recv.at[0])
    drain(mixed.at[pl.ds(0, n_tp - 1), head, :], small_recv.at[6])
    stacked = jnp.concatenate([mixed[k] for k in range(n_tp)], axis=1)
    projected = jnp.dot(stacked, w_diag[...], preferred_element_type=F32)
    projected = jnp.concatenate([projected[:, :128], projected[:, 128:]], axis=0)
    residual = (s_in[...].reshape(n_rows, 128).astype(F32) + projected).astype(BF16)
    res_keep[...] = residual
    res = residual.astype(F32)

    sums = jnp.sum(res * res, axis=1, keepdims=True)
    across = jnp.transpose(jnp.broadcast_to(sums, (n_rows, 128)))
    first_row = lax.broadcasted_iota(jnp.int32, (8, half), 0) == 0
    squares[t] = jnp.where(first_row, across[0:8, :half], across[0:8, half:])
    for step_y, other in tp_steps:
        remote(
            squares.at[t], squares.at[t], small_send.at[3], small_recv.at[2],
            tp=at_tp(step_y, other),
        ).start()
    drain(squares.at[pl.ds(0, n_tp - 1)], small_recv.at[2])
    total = squares[0]
    for k in range(1, n_tp):
        total = total + squares[k]
    scale = lax.rsqrt(total / (n_tp * 128) + EPS)
    scale = jnp.concatenate(
        [jnp.transpose(jnp.broadcast_to(scale[k : k + 1, :], (half, half))) for k in range(2)], axis=0
    )
    gains = ffn_gain[...].astype(F32).reshape(n_tp, 128)
    gain_no = lax.broadcasted_iota(jnp.int32, (n_tp, 128), 0)
    gain = jnp.sum(jnp.where(gain_no == t, gains, 0.0), axis=0, keepdims=True)
    normed = (res * scale * gain).astype(BF16)

    norms[0] = normed

    right, left = at_tp(1, False), at_tp(-1, False)
    lower, upper = zone // 2, zone - zone // 2

    def ring_step(j, d):
        kind, z, _ = OPS[j]
        base = 0 if kind == "g" else z * zone

        def part(place, span, core_no=0):
            first, size = span
            span = pl.ds(base + first, size)
            if kind == "g":
                return norms.at[place, span, :]
            return (rows if kind == "r" else hidden).at[core_no, place, span, :]

        def pass_on(origin, shifted, span, to, sem):
            remote(part(origin, span), part(shifted, span), ring_send.at[j], sem, tp=to).start()

        def cross(place, span):
            if kind != "g":
                remote(
                    part(place, span), part(place, span, 1), ring_send.at[j], ring_pair.at[j],
                    tp=partner,
                ).start()

        full, first, second = (0, zone), (0, lower), (lower, upper)
        if d == 0:
            if kind == "r":
                drain(part(0, full), far_recv.at[z - FAR[0]])
            pass_on(AT[0], AT[-1], full, right, ring_recv.at[j, 0, 0])
            pass_on(AT[0], AT[1], full, left, ring_recv.at[j, 1, 0])
            cross(AT[0], full)
            return
        for way, sign, ahead, end in ((0, -1, right, first), (1, 1, left, second)):
            origin = AT[sign * d] if d < 4 else AT[4]
            span = full if d < 4 else end
            drain(part(origin, span), ring_recv.at[j, way, d - 1])
            if d < 4:
                shifted = AT[sign * (d + 1)] if d < 3 else AT[4]
                pass_on(origin, shifted, full if d < 3 else end, ahead, ring_recv.at[j, way, d])
            cross(origin, span)
        if d == 4 and kind != "g":
            drain(
                (rows if kind == "r" else hidden).at[1, :, pl.ds(base, zone), :], ring_pair.at[j]
            )

    ring_step(0, 0)

    def expert_of(p):
        to_z = lax.rem(sz - z_step(p) + dim_z, dim_z)
        return to_z * dim_x + lax.rem(sx - p % dim_x + dim_x, dim_x)

    for z in FAR:
        base = (z - FAR[0]) * zone
        far_out[pl.ds(base, zone), :] = jnp.dot(
            picker[pl.ds(z * zone, zone), :], normed, preferred_element_type=F32
        ).astype(BF16)
        for x in range(dim_x):
            p = z * dim_x + x
            remote(
                far_out.at[pl.ds(base + x * block, block), :],
                rows.at[0, 0, pl.ds(p * block, block), :],
                small_send.at[5], far_recv.at[z - FAR[0]], sp=expert_of(p),
            ).start()

    def pick_zone(z, first, last):
        span = pl.ds(z * zone, zone)
        wide_rows = jnp.concatenate([norms[k] for k in range(first, last)], axis=1)
        picked = jnp.dot(picker[span, :], wide_rows, preferred_element_type=F32).astype(BF16)
        for k in range(first, last):
            piece = picked[:, (k - first) * 128 : (k - first + 1) * 128]
            near_out[k, span, :] = piece
            if z == 0:
                rows[0, k, pl.ds(0, block), :] = piece[:block]
        for x in range(dim_x):
            p = z * dim_x + x
            if p == 0:
                continue
            place = pl.ds(p * block, block)
            remote(
                near_out.at[pl.ds(first, last - first), place, :],
                rows.at[0, pl.ds(first, last - first), place, :],
                small_send.at[6], near_recv.at[z], sp=expert_of(p),
            ).start()

    def pick(batch):
        if batch == 0:
            for z in EARLY:
                pick_zone(z, 0, FIRST_SLICES)
            return
        if batch == 1:
            for z in EARLY:
                pick_zone(z, FIRST_SLICES, dim_y)
            return
        pick_zone(LATE[batch - 2], 0, dim_y)

    def across(z):
        own_x = 1 if z == 0 else 0
        taken = pl.ds(z * zone, zone - own_x * block)
        drain(rows.at[0, :, taken, :], near_recv.at[z])
        span = pl.ds(z * zone, zone)
        remote(
            rows.at[0, :, span, :], rows.at[1, :, span, :], small_send.at[8], near_pair.at[z],
            tp=partner,
        ).start()

    for step_y, other in tp_steps:
        to = at_tp(step_y, other)
        remote(
            res_keep.at[pl.ds(pl.multiple_of(to * own, own), own), :], res_in.at[t],
            small_send.at[4], small_recv.at[3], tp=to,
        ).start()
    res_in[t] = res_keep[pl.ds(pl.multiple_of(t * own, own), own), :]

    def fill_weights(part, carry):
        first = pl.multiple_of(part * 256, 256)
        number = lax.broadcasted_iota(jnp.int32, (n_rows, 256), 1) + part * 256
        number = number.astype(F32)
        columns = slot_cols[...]
        summed = jnp.zeros((n_rows, 256), F32)
        for k in range(top):
            summed = summed + jnp.where(
                number == columns[:, k : k + 1], columns[:, top + k : top + k + 1], 0.0
            )
        high = summed.astype(BF16)
        comb_w[pl.ds(0, n_rows), pl.ds(first, 256)] = high
        comb_w[pl.ds(n_rows, n_rows), pl.ds(first, 256)] = (summed - high.astype(F32)).astype(BF16)
        return carry

    def weights(z):
        lax.fori_loop(z * (slots // 1024), (z + 1) * (slots // 1024), fill_weights, 0)

    drain(w_gu.at[:, pl.ds(0, 128)], load_sem.at[0])
    drain(w_gu.at[:, pl.ds(128, 128)], load_sem.at[1])
    drain(w_down, load_sem.at[2])

    def stacked_rows(held, z):
        span = pl.ds(z * zone, zone)
        return jnp.concatenate(
            [held[core_no, k, span, :] for core_no in range(2) for k in range(dim_y)], axis=1
        )

    def units(z):
        span = pl.ds(z * zone, zone)
        if z in NEAR:
            drain(rows.at[1, :, span, :], near_pair.at[z])
        both = jnp.dot(stacked_rows(rows, z), w_gu[...], preferred_element_type=F32)
        gate = jnp.minimum(both[:, :128], LIMIT)
        up = jnp.clip(both[:, 128:], -LIMIT, LIMIT)
        hidden[0, 0, span, :] = ((up + 1.0) * (gate * jax.nn.sigmoid(SLOPE * gate))).astype(BF16)

    def outputs(z):
        span = pl.ds(z * zone, zone)
        done = jnp.dot(stacked_rows(hidden, z), w_down[...], preferred_element_type=F32)
        result[span, :] = done.astype(BF16)
        for x in range(dim_x):
            p = z * dim_x + x
            place = pl.ds(p * block, block)
            if p == 0:
                back[place, :] = result[place, :]
                continue
            to_z = lax.rem(sz + z_step(p), dim_z)
            to_x = lax.rem(sx + x, dim_x)
            remote(
                result.at[place, :], back.at[place, :], small_send.at[9], back_recv.at[z],
                sp=to_z * dim_x + to_x,
            ).start()

    tasks = dict(pick=pick, weights=weights, across=across, units=units)
    for slot in range(max(op[2] for op in OPS) + 5):
        finished = []
        for j, (kind, z, start) in reversed(list(enumerate(OPS))):
            d = slot - start
            if 0 <= d <= 4 and (j, d) != (0, 0):
                ring_step(j, d)
                if d == 4 and kind == "h":
                    finished.append(z)
        for name, z in WORK.get(slot, ()):
            tasks[name](z)
        for z in finished:
            outputs(z)

    summed = jnp.zeros((2 * n_rows, 128), F32)
    for z in [op[1] for op in OPS if op[0] == "h"]:
        taken = zone - (block if z == 0 else 0)
        drain(back.at[pl.ds(0, taken), :], back_recv.at[z])
        span = pl.ds(z * zone, zone)
        summed = summed + jnp.dot(comb_w[:, span], back[span, :], preferred_element_type=F32)
    comb_out[...] = (summed[:n_rows] + summed[n_rows:]).astype(BF16)
    for step_y, other in tp_steps:
        to = at_tp(step_y, other)
        remote(
            comb_out.at[pl.ds(pl.multiple_of(to * own, own), own), :], comb_in.at[t],
            small_send.at[7], small_recv.at[4], tp=to,
        ).start()
    comb_in[t] = comb_out[pl.ds(pl.multiple_of(t * own, own), own), :]

    halo.wait_send()
    drain(w_in.at[0, pl.ds(0, n_tp - 1)], small_send.at[0])
    drain(w_in.at[pl.ds(0, dim_x - 1)], small_send.at[10])
    drain(s_in.at[pl.ds(0, n_tp - 1)], small_send.at[1])
    drain(mixed.at[pl.ds(0, 2 * dim_y - 1), body, :], small_send.at[2])
    drain(mixed.at[pl.ds(0, n_tp - 1), head, :], small_send.at[11])
    drain(squares.at[pl.ds(0, n_tp - 1)], small_send.at[3])
    drain(res_in.at[pl.ds(0, n_tp - 1)], small_send.at[4])
    drain(far_out, small_send.at[5])
    drain(near_out.at[:, pl.ds(0, len(NEAR) * zone - block), :], small_send.at[6])
    drain(near_out, small_send.at[8])
    drain(result.at[pl.ds(0, slots - block), :], small_send.at[9])
    for j, op in enumerate(OPS):
        if op[0] == "g":
            drain(norms.at[pl.ds(0, 7)], ring_send.at[j])
        else:
            drain(rows.at[0, pl.ds(0, 3), pl.ds(0, 5 * zone), :], ring_send.at[j])

    drain(res_in.at[pl.ds(0, n_tp - 1)], small_recv.at[3])
    drain(comb_in.at[pl.ds(0, n_tp - 1)], small_recv.at[4])
    drain(comb_in.at[pl.ds(0, n_tp - 1)], small_send.at[7])
    combined = jnp.concatenate([comb_in[k] for k in range(n_tp)], axis=1).astype(F32)
    kept = jnp.concatenate([res_in[k] for k in range(n_tp)], axis=1).astype(F32)
    mean = jnp.mean(combined * combined, axis=1, keepdims=True)
    out[...] = (kept + combined * lax.rsqrt(mean + EPS) * post_gain[...].astype(F32)[None, :]).astype(BF16)


def local(
    stream_in, pre_gate, value_in, post_gate, conv_taps, out_weight, route_ids, route_weight,
    ffn_gain, post_gain, gate_proj, up_proj, down_proj,
):
    n_sp, n_tp = lax.axis_size("sp"), lax.axis_size("tp")
    own, features = stream_in.shape
    n_rows = pre_gate.shape[0]
    cap = 2 * own * route_ids.shape[1] // n_sp
    slots = n_sp * n_tp * cap
    vmem = pl.BlockSpec(memory_space=pltpu.VMEM)
    hbm = pl.BlockSpec(memory_space=pl.ANY)
    dma = pltpu.SemaphoreType.DMA
    zone = 4 * n_tp * cap
    half_tp = n_tp // 2
    return pl.pallas_call(
        functools.partial(kernel, (n_sp, n_tp, 4, cap)),
        out_shape=jax.ShapeDtypeStruct(stream_in.shape, BF16),
        in_specs=[hbm] * 13,
        out_specs=vmem,
        scratch_shapes=[
            pltpu.VMEM(stream_in.shape, BF16),
            pltpu.VMEM(pre_gate.shape[::-1], BF16),
            pltpu.VMEM(pre_gate.shape[::-1], BF16),
            pltpu.VMEM(pre_gate.shape[::-1], BF16),
            pltpu.VMEM(conv_taps.shape, BF16),
            pltpu.VMEM(out_weight.shape, BF16),
            pltpu.VMEM(route_ids.shape[::-1], jnp.int32),
            pltpu.VMEM(route_weight.shape[::-1], F32),
            pltpu.VMEM(ffn_gain.shape, BF16),
            pltpu.VMEM(post_gain.shape, BF16),
            dma((10,)),
            pltpu.VMEM((16, 128), BF16),
            pltpu.VMEM((16, 128), BF16),
            pltpu.VMEM((n_tp, n_rows // 2, 128), BF16),
            pltpu.VMEM((4, n_tp, 16, 128), BF16),
            pltpu.VMEM((n_tp * 128, 256), BF16),
            pltpu.VMEM((n_tp, own, 128), BF16),
            pltpu.VMEM((n_tp, 8, n_rows // 2), F32),
            pltpu.VMEM((slots, n_rows), BF16),
            pltpu.VMEM((2 * n_rows, slots), BF16),
            pltpu.VMEM((128, n_rows), F32),
            pltpu.VMEM((n_rows, 128), F32),
            pltpu.VMEM((half_tp, n_rows, 128), BF16),
            pltpu.VMEM((len(FAR) * zone, 128), BF16),
            pltpu.VMEM((half_tp, len(NEAR) * zone, 128), BF16),
            pltpu.VMEM((2, half_tp, slots, 128), BF16),
            pltpu.VMEM((2, half_tp, slots, 128), BF16),
            pltpu.VMEM((slots, 128), BF16),
            pltpu.VMEM((slots, 128), BF16),
            pltpu.VMEM((n_rows, 128), BF16),
            pltpu.VMEM((n_tp, own, 128), BF16),
            pltpu.VMEM((n_rows, 128), BF16),
            pltpu.VMEM((n_tp, own, 128), BF16),
            pltpu.VMEM((features, 256), BF16),
            pltpu.VMEM((features, 128), BF16),
            dma((3,)), dma((2,)), dma((12,)), dma((7,)), dma((8,)), dma((len(FAR),)),
            dma((len(NEAR),)), dma((len(NEAR),)),
            dma((len(OPS), 2, 4)), dma((len(OPS),)), dma((len(OPS),)), dma((8,)),
        ],
        compiler_params=pltpu.CompilerParams(
            collective_id=0, has_side_effects=True, vmem_limit_bytes=63 * 1024 * 1024
        ),
        cost_estimate=pl.CostEstimate(flops=4 * 10**9, bytes_accessed=3 * 10**6, transcendentals=0),
    )(
        stream_in, pre_gate.T, value_in.T, post_gate.T, conv_taps, out_weight,
        route_ids.T, route_weight.T,
        ffn_gain, post_gain,
        gate_proj, up_proj, down_proj,
    )


def solution(mesh):
    placed = (
        P(("sp", "tp"), None),
        P("sp", "tp"),
        P("sp", "tp"),
        P("sp", "tp"),
        P(None, "tp"),
        P("tp", None),
        P("sp", None),
        P("sp", None),
        P(),
        P(),
        P("sp", None, "tp"),
        P("sp", None, "tp"),
        P("sp", None, "tp"),
    )
    return jax.shard_map(
        local, mesh=mesh, in_specs=placed, out_specs=P(("sp", "tp"), None), check_vma=False
    )
```

```python
import functools

import jax
import jax.numpy as jnp
from jax import lax
from jax.experimental import pallas as pl
from jax.experimental.pallas import tpu as pltpu
from jax.sharding import PartitionSpec as P

MESH = pl.DeviceIdType.MESH
F32 = jnp.float32
BF16 = jnp.bfloat16
LIMIT = 7.0
SLOPE = 1.702
EPS = 1e-06
OFFSETS = (0, 1, -1, 2, -2, 3, -3, 4)
AT = {offset: place for place, offset in enumerate(OFFSETS)}
NEAR, FAR = (0, 1, 2, 3, 4), (5, 6, 7)
EARLY, LATE = (0, 1, 2), (3, 4)
FIRST_SLICES = 3
OPS = (('g', 0, 0), ('r', 5, 2), ('r', 6, 3), ('r', 7, 6), ('h', 5, 7), ('h', 6, 8), ('h', 0, 9), ('h', 1, 10), ('h', 7, 11), ('h', 2, 12), ('h', 3, 13), ('h', 4, 13))
WORK = {1: [('pick', 0)], 4: [('pick', 1)], 5: [('pick', 2)], 6: [('pick', 3), ('units', 5)], 13: [('weights', 0), ('weights', 1)], 14: [('weights', 2), ('weights', 3)], 7: [('units', 6), ('across', 0)], 8: [('units', 0), ('across', 1)], 9: [('units', 1)], 10: [('units', 7), ('across', 2)], 11: [('units', 2), ('across', 3), ('across', 4)], 12: [('units', 3), ('units', 4)]}


def kernel(
    cfg,
    stream_hbm, pre_hbm, value_hbm, post_hbm, taps_hbm, weight_hbm, ids_hbm, route_w_hbm,
    ffn_gain_hbm, post_gain_hbm, gate_hbm, up_hbm, down_hbm,
    out,
    stream, pre, value, post, taps, weight, ids, route_w, ffn_gain, post_gain, in_sem,
    halo_src, halo_dst, mixed, w_in, w_diag, s_in, squares, picker, comb_w, aux, slot_cols,
    norms, far_out, near_out, rows, hidden, result, back, res_keep, res_in, comb_out, comb_in, w_gu, w_down,
    load_sem, halo_sem, small_send, small_recv, mix_recv, far_recv, near_recv, near_pair,
    ring_recv, ring_pair, ring_send, back_recv,
):
    n_sp, n_tp, dim_x, cap = cfg
    dim_z, dim_y = n_sp // dim_x, n_tp // 2
    s, t = lax.axis_index("sp"), lax.axis_index("tp")
    sz, sx = s // dim_x, lax.rem(s, dim_x)
    y, core = t // 2, lax.rem(t, 2)
    n_rows = pre.shape[1]
    channels = pre.shape[0]
    top = ids.shape[0]
    own = n_rows // n_tp
    half = n_rows // 2
    block = own * cap * n_tp // own
    slots = block * n_sp
    zone = dim_x * block

    def at_tp(step_y, other_core):
        to_core = 1 - core if other_core else core
        return lax.rem(y + step_y + dim_y, dim_y) * 2 + to_core

    def remote(src, dst, send, recv, tp=None, sp=None):
        target = {"tp": tp} if sp is None else {"sp": sp}
        return pltpu.make_async_remote_copy(
            src_ref=src, dst_ref=dst, send_sem=send, recv_sem=recv,
            device_id=target, device_id_type=MESH,
        )

    def drain(ref, sem):
        pltpu.make_async_copy(ref, ref, sem).wait()

    def z_step(p):
        place = p // dim_x
        return (place + 1) // 2 if place % 2 else (dim_z - place // 2) % dim_z

    barrier = pltpu.get_barrier_semaphore()

    def greet_tp(step, carry):
        pl.semaphore_signal(
            barrier, inc=1, device_id={"tp": lax.rem(t + step, n_tp)}, device_id_type=MESH
        )
        return carry

    def greet_sp(step, carry):
        pl.semaphore_signal(
            barrier, inc=1, device_id={"sp": lax.rem(s + step, n_sp)}, device_id_type=MESH
        )
        return carry

    lax.fori_loop(n_sp // 4, n_sp - n_sp // 4, greet_sp, 0)
    lax.fori_loop(1, n_tp, greet_tp, 0)
    lax.fori_loop(1, n_sp // 4, greet_sp, 0)
    lax.fori_loop(n_sp - n_sp // 4, n_sp, greet_sp, 0)

    inputs = [
        pltpu.make_async_copy(there, here, in_sem.at[k])
        for k, (there, here) in enumerate((
            (pre_hbm, pre), (value_hbm, value), (post_hbm, post), (weight_hbm, weight),
            (taps_hbm, taps), (stream_hbm, stream), (ids_hbm, ids), (route_w_hbm, route_w),
            (ffn_gain_hbm, ffn_gain), (post_gain_hbm, post_gain),
        ))
    ]
    for copy in inputs:
        copy.start()
    for copy in inputs[:3]:
        copy.wait()

    gated = (pre[...].astype(F32) * value[...].astype(F32)).astype(BF16).astype(F32)
    gates = jnp.transpose(jnp.concatenate([gated, post[...].astype(F32)], axis=0))
    halo_src[...] = gates[n_rows - 16 :, :].astype(BF16)

    for copy in inputs[3:]:
        copy.wait()
    pl.semaphore_wait(barrier, n_tp + n_sp - 2)

    halo = remote(
        halo_src, halo_dst, halo_sem.at[0], halo_sem.at[1], sp=lax.rem(s + 1, n_sp)
    )
    halo.start()

    share = weight.shape[0] // dim_x
    quarter = pl.ds(pl.multiple_of(sx * share, share), share)
    tp_steps = [(d, o) for d in (4, 3, 5, 2, 6, 1, 7) for o in (False, True)] + [(0, True)]
    for step_y, other in tp_steps:
        to = at_tp(step_y, other)
        piece = pl.ds(pl.multiple_of(to * 128, 128), 128)
        remote(
            weight.at[quarter, piece], w_in.at[sx, t], small_send.at[0], small_recv.at[0], tp=to
        ).start()
    own_cols = pl.ds(pl.multiple_of(t * 128, 128), 128)
    w_in[sx, t] = weight[quarter, own_cols]
    s_in[t] = stream[:, own_cols]

    wide, second = gates[:, :channels], gates[:, channels:]
    tap = taps[...].astype(F32)
    shift_1, shift_2 = pltpu.roll(wide, 1, 0), pltpu.roll(wide, 2, 0)

    def mixer_rows(two_back, one_back, here, gate):
        convolved = tap[0:1] * two_back
        convolved = convolved + tap[1:2] * one_back
        convolved = convolved + tap[2:3] * here
        return gate * convolved

    mixer = mixer_rows(shift_2, shift_1, wide, second)
    body = pl.ds(16, half - 16)
    head = pl.ds(0, 16)
    mixed[t, body, :] = jnp.concatenate([mixer[16:half], mixer[half + 16 :]], axis=1).astype(BF16)

    steps = (4, 3, 5, 2, 6, 1, 7)
    own_body = mixed.at[t, body, :]
    for step_y in steps:
        remote(
            own_body, own_body, small_send.at[2], mix_recv.at[step_y], tp=at_tp(step_y, False)
        ).start()
    partner = at_tp(0, True)
    remote(own_body, own_body, small_send.at[2], mix_recv.at[0], tp=partner).start()
    for step_y, other in tp_steps:
        to = at_tp(step_y, other)
        piece = pl.ds(pl.multiple_of(to * 128, 128), 128)
        remote(stream.at[:, piece], s_in.at[t], small_send.at[1], small_recv.at[1], tp=to).start()
    aux[...] = jnp.zeros_like(aux)
    aux[0:top, :] = ids[...].astype(F32)
    aux[top : 2 * top, :] = route_w[...]
    by_row = jnp.transpose(aux[...])
    id_cols = [by_row[:, k : k + 1] for k in range(top)]
    amounts = [by_row[:, top + k : top + k + 1] for k in range(top)]
    lane = lax.broadcasted_iota(jnp.int32, (n_rows, 128), 1)
    lane_f = lane.astype(F32)
    named = jnp.zeros((n_rows, 128), F32)
    for k in range(top):
        named = named + jnp.where(id_cols[k] == lane_f, 1.0, 0.0)
    row_a = lax.broadcasted_iota(jnp.int32, (n_rows, n_rows), 0)
    row_b = lax.broadcasted_iota(jnp.int32, (n_rows, n_rows), 1)
    earlier = jnp.where((row_a > row_b) & (row_a // own == row_b // own), 1.0, 0.0).astype(BF16)
    rank = jnp.dot(earlier, named.astype(BF16), preferred_element_type=F32)
    dz = lax.rem(sz - lane // dim_x + 32 * dim_z, dim_z)
    dx = lax.rem(sx - lax.rem(lane, dim_x) + 32 * dim_x, dim_x)
    z_place = jnp.where(dz * 2 <= dim_z, jnp.maximum(2 * dz - 1, 0), 2 * (dim_z - dz))
    at_row = lax.broadcasted_iota(jnp.int32, (n_rows, 128), 0)
    slot_of = ((z_place * dim_x + dx) * block + (at_row // own) * cap).astype(F32) + rank
    places = [
        jnp.sum(jnp.where(id_cols[k] == lane_f, slot_of, 0.0), axis=1, keepdims=True)
        for k in range(top)
    ]
    columns = jnp.zeros((n_rows, 128), F32)
    for k in range(top):
        columns = jnp.where(lane == k, places[k], columns)
        columns = jnp.where(lane == top + k, amounts[k], columns)
    slot_cols[...] = columns
    slot_rows = jnp.transpose(columns)
    w_diag[...] = jnp.zeros_like(w_diag)

    row_no = lax.broadcasted_iota(jnp.int32, (16, channels), 0)
    halo.wait_recv()
    rim = halo_dst[...].astype(F32)[:, :channels]
    rim = jnp.where(s > 0, rim, 0.0)
    last, before_last = rim[15:16, :], rim[14:15, :]
    one_back = jnp.where(row_no == 0, last, shift_1[:16])
    two_back = jnp.where(row_no == 0, before_last, jnp.where(row_no == 1, last, shift_2[:16]))
    first_rows = mixer_rows(two_back, one_back, wide[:16], second[:16])
    mixed[t, head, :] = jnp.concatenate([first_rows, mixer[half : half + 16]], axis=1).astype(BF16)
    own_head = mixed.at[t, head, :]
    for step_y, other in tp_steps:
        remote(
            own_head, own_head, small_send.at[11], small_recv.at[6], tp=at_tp(step_y, other)
        ).start()
    for core_no in range(2):
        for place, offset in enumerate(OFFSETS):
            origin = pl.ds(pl.multiple_of(at_tp(offset, core_no == 1) * 128, 128), 128)
            here = pl.ds((core_no * dim_y + place) * 128, 128)
            pltpu.make_async_copy(
                gate_hbm.at[0, origin, :], w_gu.at[here, pl.ds(0, 128)], load_sem.at[0]
            ).start()
            pltpu.make_async_copy(
                up_hbm.at[0, origin, :], w_gu.at[here, pl.ds(128, 128)], load_sem.at[1]
            ).start()
            pltpu.make_async_copy(
                down_hbm.at[0, origin, :], w_down.at[here, :], load_sem.at[2]
            ).start()

    drain(w_in.at[sx, pl.ds(0, n_tp - 1)], small_recv.at[0])
    for step_x in (2, 1, 3):
        remote(
            w_in.at[sx], w_in.at[sx], small_send.at[10], small_recv.at[5],
            sp=sz * dim_x + lax.rem(sx + step_x, dim_x),
        ).start()

    def fill_picker(part, carry):
        first = pl.multiple_of(part * 256, 256)
        number = lax.broadcasted_iota(jnp.int32, (256, n_rows), 0) + part * 256
        number = number.astype(F32)
        hit = number == slot_rows[0:1, :]
        for k in range(1, top):
            hit = hit | (number == slot_rows[k : k + 1, :])
        picker[pl.ds(first, 256), :] = jnp.where(hit, 1.0, 0.0).astype(BF16)
        return carry

    lax.fori_loop(0, slots // 256, fill_picker, 0)

    drain(w_in.at[pl.ds(0, dim_x - 1)], small_recv.at[5])
    for k in range(n_tp):
        piece = jnp.concatenate([w_in[x, k] for x in range(dim_x)], axis=0)
        w_diag[pl.ds(k * 128, 64), pl.ds(0, 128)] = piece
        w_diag[pl.ds(k * 128 + 64, 64), pl.ds(128, 128)] = piece
    for step_y in steps:
        arrived = mixed.at[at_tp(-step_y, False), body, :]
        drain(arrived, mix_recv.at[step_y])
        remote(arrived, arrived, small_send.at[2], mix_recv.at[0], tp=partner).start()
    drain(s_in.at[pl.ds(0, n_tp - 1)], small_recv.at[1])
    drain(mixed.at[pl.ds(0, dim_y), body, :], mix_recv.at[0])
    drain(mixed.at[pl.ds(0, n_tp - 1), head, :], small_recv.at[6])
    stacked = jnp.concatenate([mixed[k] for k in range(n_tp)], axis=1)
    projected = jnp.dot(stacked, w_diag[...], preferred_element_type=F32)
    projected = jnp.concatenate([projected[:, :128], projected[:, 128:]], axis=0)
    residual = (s_in[...].reshape(n_rows, 128).astype(F32) + projected).astype(BF16)
    res_keep[...] = residual
    res = residual.astype(F32)

    sums = jnp.sum(res * res, axis=1, keepdims=True)
    across = jnp.transpose(jnp.broadcast_to(sums, (n_rows, 128)))
    first_row = lax.broadcasted_iota(jnp.int32, (8, half), 0) == 0
    squares[t] = jnp.where(first_row, across[0:8, :half], across[0:8, half:])
    for step_y, other in tp_steps:
        remote(
            squares.at[t], squares.at[t], small_send.at[3], small_recv.at[2],
            tp=at_tp(step_y, other),
        ).start()
    drain(squares.at[pl.ds(0, n_tp - 1)], small_recv.at[2])
    total = squares[0]
    for k in range(1, n_tp):
        total = total + squares[k]
    scale = lax.rsqrt(total / (n_tp * 128) + EPS)
    scale = jnp.concatenate(
        [jnp.transpose(jnp.broadcast_to(scale[k : k + 1, :], (half, half))) for k in range(2)], axis=0
    )
    gains = ffn_gain[...].astype(F32).reshape(n_tp, 128)
    gain_no = lax.broadcasted_iota(jnp.int32, (n_tp, 128), 0)
    gain = jnp.sum(jnp.where(gain_no == t, gains, 0.0), axis=0, keepdims=True)
    normed = (res * scale * gain).astype(BF16)

    norms[0] = normed

    right, left = at_tp(1, False), at_tp(-1, False)
    lower, upper = zone // 2, zone - zone // 2

    def ring_step(j, d):
        kind, z, _ = OPS[j]
        base = 0 if kind == "g" else z * zone

        def part(place, span, core_no=0):
            first, size = span
            span = pl.ds(base + first, size)
            if kind == "g":
                return norms.at[place, span, :]
            return (rows if kind == "r" else hidden).at[core_no, place, span, :]

        def pass_on(origin, shifted, span, to, sem):
            remote(part(origin, span), part(shifted, span), ring_send.at[j], sem, tp=to).start()

        def cross(place, span):
            if kind != "g":
                remote(
                    part(place, span), part(place, span, 1), ring_send.at[j], ring_pair.at[j],
                    tp=partner,
                ).start()

        full, first, second = (0, zone), (0, lower), (lower, upper)
        if d == 0:
            if kind == "r":
                drain(part(0, full), far_recv.at[z - FAR[0]])
            pass_on(AT[0], AT[-1], full, right, ring_recv.at[j, 0, 0])
            pass_on(AT[0], AT[1], full, left, ring_recv.at[j, 1, 0])
            cross(AT[0], full)
            return
        for way, sign, ahead, end in ((0, -1, right, first), (1, 1, left, second)):
            origin = AT[sign * d] if d < 4 else AT[4]
            span = full if d < 4 else end
            drain(part(origin, span), ring_recv.at[j, way, d - 1])
            if d < 4:
                shifted = AT[sign * (d + 1)] if d < 3 else AT[4]
                pass_on(origin, shifted, full if d < 3 else end, ahead, ring_recv.at[j, way, d])
            cross(origin, span)
        if d == 4 and kind != "g":
            drain(
                (rows if kind == "r" else hidden).at[1, :, pl.ds(base, zone), :], ring_pair.at[j]
            )

    ring_step(0, 0)

    def expert_of(p):
        to_z = lax.rem(sz - z_step(p) + dim_z, dim_z)
        return to_z * dim_x + lax.rem(sx - p % dim_x + dim_x, dim_x)

    for z in FAR:
        base = (z - FAR[0]) * zone
        far_out[pl.ds(base, zone), :] = jnp.dot(
            picker[pl.ds(z * zone, zone), :], normed, preferred_element_type=F32
        ).astype(BF16)
        for x in range(dim_x):
            p = z * dim_x + x
            remote(
                far_out.at[pl.ds(base + x * block, block), :],
                rows.at[0, 0, pl.ds(p * block, block), :],
                small_send.at[5], far_recv.at[z - FAR[0]], sp=expert_of(p),
            ).start()

    def pick_zone(z, first, last):
        span = pl.ds(z * zone, zone)
        wide_rows = jnp.concatenate([norms[k] for k in range(first, last)], axis=1)
        picked = jnp.dot(picker[span, :], wide_rows, preferred_element_type=F32).astype(BF16)
        for k in range(first, last):
            piece = picked[:, (k - first) * 128 : (k - first + 1) * 128]
            near_out[k, span, :] = piece
            if z == 0:
                rows[0, k, pl.ds(0, block), :] = piece[:block]
        for x in range(dim_x):
            p = z * dim_x + x
            if p == 0:
                continue
            place = pl.ds(p * block, block)
            remote(
                near_out.at[pl.ds(first, last - first), place, :],
                rows.at[0, pl.ds(first, last - first), place, :],
                small_send.at[6], near_recv.at[z], sp=expert_of(p),
            ).start()

    def pick(batch):
        if batch == 0:
            for z in EARLY:
                pick_zone(z, 0, FIRST_SLICES)
            return
        if batch == 1:
            for z in EARLY:
                pick_zone(z, FIRST_SLICES, dim_y)
            return
        pick_zone(LATE[batch - 2], 0, dim_y)

    def across(z):
        own_x = 1 if z == 0 else 0
        taken = pl.ds(z * zone, zone - own_x * block)
        drain(rows.at[0, :, taken, :], near_recv.at[z])
        span = pl.ds(z * zone, zone)
        remote(
            rows.at[0, :, span, :], rows.at[1, :, span, :], small_send.at[8], near_pair.at[z],
            tp=partner,
        ).start()

    for step_y, other in tp_steps:
        to = at_tp(step_y, other)
        remote(
            res_keep.at[pl.ds(pl.multiple_of(to * own, own), own), :], res_in.at[t],
            small_send.at[4], small_recv.at[3], tp=to,
        ).start()
    res_in[t] = res_keep[pl.ds(pl.multiple_of(t * own, own), own), :]

    def fill_weights(part, carry):
        first = pl.multiple_of(part * 256, 256)
        number = lax.broadcasted_iota(jnp.int32, (n_rows, 256), 1) + part * 256
        number = number.astype(F32)
        columns = slot_cols[...]
        summed = jnp.zeros((n_rows, 256), F32)
        for k in range(top):
            summed = summed + jnp.where(
                number == columns[:, k : k + 1], columns[:, top + k : top + k + 1], 0.0
            )
        high = summed.astype(BF16)
        comb_w[pl.ds(0, n_rows), pl.ds(first, 256)] = high
        comb_w[pl.ds(n_rows, n_rows), pl.ds(first, 256)] = (summed - high.astype(F32)).astype(BF16)
        return carry

    def weights(z):
        lax.fori_loop(z * (slots // 1024), (z + 1) * (slots // 1024), fill_weights, 0)

    drain(w_gu.at[:, pl.ds(0, 128)], load_sem.at[0])
    drain(w_gu.at[:, pl.ds(128, 128)], load_sem.at[1])
    drain(w_down, load_sem.at[2])

    def stacked_rows(held, z):
        span = pl.ds(z * zone, zone)
        return jnp.concatenate(
            [held[core_no, k, span, :] for core_no in range(2) for k in range(dim_y)], axis=1
        )

    def units(z):
        span = pl.ds(z * zone, zone)
        if z in NEAR:
            drain(rows.at[1, :, span, :], near_pair.at[z])
        both = jnp.dot(stacked_rows(rows, z), w_gu[...], preferred_element_type=F32)
        gate = jnp.minimum(both[:, :128], LIMIT)
        up = jnp.clip(both[:, 128:], -LIMIT, LIMIT)
        hidden[0, 0, span, :] = ((up + 1.0) * (gate * jax.nn.sigmoid(SLOPE * gate))).astype(BF16)

    def outputs(z):
        span = pl.ds(z * zone, zone)
        done = jnp.dot(stacked_rows(hidden, z), w_down[...], preferred_element_type=F32)
        result[span, :] = done.astype(BF16)
        for x in range(dim_x):
            p = z * dim_x + x
            place = pl.ds(p * block, block)
            if p == 0:
                back[place, :] = result[place, :]
                continue
            to_z = lax.rem(sz + z_step(p), dim_z)
            to_x = lax.rem(sx + x, dim_x)
            remote(
                result.at[place, :], back.at[place, :], small_send.at[9], back_recv.at[z],
                sp=to_z * dim_x + to_x,
            ).start()

    tasks = dict(pick=pick, weights=weights, across=across, units=units)
    last_slot = max(op[2] for op in OPS) + 4
    for slot in range(last_slot + 1):
        finished = []
        for j, (kind, z, start) in reversed(list(enumerate(OPS))):
            d = slot - start
            if 0 <= d <= 4 and (j, d) != (0, 0):
                ring_step(j, d)
                if d == 4 and kind == "h":
                    if slot == last_slot:
                        outputs(z)
                    else:
                        finished.append(z)
        for name, z in WORK.get(slot, ()):
            tasks[name](z)
        for z in finished:
            outputs(z)

    summed = jnp.zeros((2 * n_rows, 128), F32)
    for z in [op[1] for op in OPS if op[0] == "h"]:
        taken = zone - (block if z == 0 else 0)
        drain(back.at[pl.ds(0, taken), :], back_recv.at[z])
        span = pl.ds(z * zone, zone)
        summed = summed + jnp.dot(comb_w[:, span], back[span, :], preferred_element_type=F32)
    comb_out[...] = (summed[:n_rows] + summed[n_rows:]).astype(BF16)
    for step_y, other in tp_steps:
        to = at_tp(step_y, other)
        remote(
            comb_out.at[pl.ds(pl.multiple_of(to * own, own), own), :], comb_in.at[t],
            small_send.at[7], small_recv.at[4], tp=to,
        ).start()
    comb_in[t] = comb_out[pl.ds(pl.multiple_of(t * own, own), own), :]

    halo.wait_send()
    drain(w_in.at[0, pl.ds(0, n_tp - 1)], small_send.at[0])
    drain(w_in.at[pl.ds(0, dim_x - 1)], small_send.at[10])
    drain(s_in.at[pl.ds(0, n_tp - 1)], small_send.at[1])
    drain(mixed.at[pl.ds(0, 2 * dim_y - 1), body, :], small_send.at[2])
    drain(mixed.at[pl.ds(0, n_tp - 1), head, :], small_send.at[11])
    drain(squares.at[pl.ds(0, n_tp - 1)], small_send.at[3])
    drain(res_in.at[pl.ds(0, n_tp - 1)], small_send.at[4])
    drain(far_out, small_send.at[5])
    drain(near_out.at[:, pl.ds(0, len(NEAR) * zone - block), :], small_send.at[6])
    drain(near_out, small_send.at[8])
    drain(result.at[pl.ds(0, slots - block), :], small_send.at[9])
    for j, op in enumerate(OPS):
        if op[0] == "g":
            drain(norms.at[pl.ds(0, 7)], ring_send.at[j])
        else:
            drain(rows.at[0, pl.ds(0, 3), pl.ds(0, 5 * zone), :], ring_send.at[j])

    drain(res_in.at[pl.ds(0, n_tp - 1)], small_recv.at[3])
    drain(comb_in.at[pl.ds(0, n_tp - 1)], small_recv.at[4])
    drain(comb_in.at[pl.ds(0, n_tp - 1)], small_send.at[7])
    combined = jnp.concatenate([comb_in[k] for k in range(n_tp)], axis=1).astype(F32)
    kept = jnp.concatenate([res_in[k] for k in range(n_tp)], axis=1).astype(F32)
    mean = jnp.mean(combined * combined, axis=1, keepdims=True)
    out[...] = (kept + combined * lax.rsqrt(mean + EPS) * post_gain[...].astype(F32)[None, :]).astype(BF16)


def local(
    stream_in, pre_gate, value_in, post_gate, conv_taps, out_weight, route_ids, route_weight,
    ffn_gain, post_gain, gate_proj, up_proj, down_proj,
):
    n_sp, n_tp = lax.axis_size("sp"), lax.axis_size("tp")
    own, features = stream_in.shape
    n_rows = pre_gate.shape[0]
    cap = 2 * own * route_ids.shape[1] // n_sp
    slots = n_sp * n_tp * cap
    vmem = pl.BlockSpec(memory_space=pltpu.VMEM)
    hbm = pl.BlockSpec(memory_space=pl.ANY)
    dma = pltpu.SemaphoreType.DMA
    zone = 4 * n_tp * cap
    half_tp = n_tp // 2
    return pl.pallas_call(
        functools.partial(kernel, (n_sp, n_tp, 4, cap)),
        out_shape=jax.ShapeDtypeStruct(stream_in.shape, BF16),
        in_specs=[hbm] * 13,
        out_specs=vmem,
        scratch_shapes=[
            pltpu.VMEM(stream_in.shape, BF16),
            pltpu.VMEM(pre_gate.shape[::-1], BF16),
            pltpu.VMEM(pre_gate.shape[::-1], BF16),
            pltpu.VMEM(pre_gate.shape[::-1], BF16),
            pltpu.VMEM(conv_taps.shape, BF16),
            pltpu.VMEM(out_weight.shape, BF16),
            pltpu.VMEM(route_ids.shape[::-1], jnp.int32),
            pltpu.VMEM(route_weight.shape[::-1], F32),
            pltpu.VMEM(ffn_gain.shape, BF16),
            pltpu.VMEM(post_gain.shape, BF16),
            dma((10,)),
            pltpu.VMEM((16, 128), BF16),
            pltpu.VMEM((16, 128), BF16),
            pltpu.VMEM((n_tp, n_rows // 2, 128), BF16),
            pltpu.VMEM((4, n_tp, 16, 128), BF16),
            pltpu.VMEM((n_tp * 128, 256), BF16),
            pltpu.VMEM((n_tp, own, 128), BF16),
            pltpu.VMEM((n_tp, 8, n_rows // 2), F32),
            pltpu.VMEM((slots, n_rows), BF16),
            pltpu.VMEM((2 * n_rows, slots), BF16),
            pltpu.VMEM((128, n_rows), F32),
            pltpu.VMEM((n_rows, 128), F32),
            pltpu.VMEM((half_tp, n_rows, 128), BF16),
            pltpu.VMEM((len(FAR) * zone, 128), BF16),
            pltpu.VMEM((half_tp, len(NEAR) * zone, 128), BF16),
            pltpu.VMEM((2, half_tp, slots, 128), BF16),
            pltpu.VMEM((2, half_tp, slots, 128), BF16),
            pltpu.VMEM((slots, 128), BF16),
            pltpu.VMEM((slots, 128), BF16),
            pltpu.VMEM((n_rows, 128), BF16),
            pltpu.VMEM((n_tp, own, 128), BF16),
            pltpu.VMEM((n_rows, 128), BF16),
            pltpu.VMEM((n_tp, own, 128), BF16),
            pltpu.VMEM((features, 256), BF16),
            pltpu.VMEM((features, 128), BF16),
            dma((3,)), dma((2,)), dma((12,)), dma((7,)), dma((8,)), dma((len(FAR),)),
            dma((len(NEAR),)), dma((len(NEAR),)),
            dma((len(OPS), 2, 4)), dma((len(OPS),)), dma((len(OPS),)), dma((8,)),
        ],
        compiler_params=pltpu.CompilerParams(
            collective_id=0, has_side_effects=True, vmem_limit_bytes=63 * 1024 * 1024
        ),
        cost_estimate=pl.CostEstimate(flops=4 * 10**9, bytes_accessed=3 * 10**6, transcendentals=0),
    )(
        stream_in, pre_gate.T, value_in.T, post_gate.T, conv_taps, out_weight,
        route_ids.T, route_weight.T,
        ffn_gain, post_gain,
        gate_proj, up_proj, down_proj,
    )


def solution(mesh):
    placed = (
        P(("sp", "tp"), None),
        P("sp", "tp"),
        P("sp", "tp"),
        P("sp", "tp"),
        P(None, "tp"),
        P("tp", None),
        P("sp", None),
        P("sp", None),
        P(),
        P(),
        P("sp", None, "tp"),
        P("sp", None, "tp"),
        P("sp", None, "tp"),
    )
    return jax.shard_map(
        local, mesh=mesh, in_specs=placed, out_specs=P(("sp", "tp"), None), check_vma=False
    )
```
